32 devices in a mesh: sp: 8 (over z, x), tp: 4 (over y, core).
Axes of the slice: x: 2, y: 2, z: 4, core: 2. Of those that a mesh axis runs over, the one named last changes fastest.
Arguments:
- queries: bfloat16 [512, 1024], P('tp', 'sp'), may hold values from -6 to 6
- input_key_matrix: bfloat16 [512, 1024], P('tp', 'sp'), may hold values from -6 to 6
- input_value_matrix: bfloat16 [1024, 1024], P('tp', 'sp'), may hold values from -6 to 6
- decay_preactivation: bfloat16 [512, 1024], P('tp', 'sp'), may hold values from -6 to 6
- extra_log_decay: float32 [512, 1024], P('tp', 'sp'), may hold values from -1 to 0, as said below
- channel_decay_speed: float32 [512], P('tp'), may hold values from 0 to 1, as said below
- output_weight_matrix: bfloat16 [2048, 1024], P(None, 'tp'), may hold values from -0.1875 to 0.1875
- stored_expert_rows: bfloat16 [1024, 2048], P('sp', 'tp'), may hold values from -6 to 6
- chosen_expert_index: int32 [1024, 2], P('sp'), may hold values from 0 to 7, all different within a row; in each aligned block of 128 rows (0 to 127, 128 to 255, ...) at most 48 rows name the same one
- expert_combine_weight: float32 [1024, 2], P('sp'), may hold values from 0.2 to 1
- cotangent: bfloat16 [1024, 2048], P('sp', 'tp'), may hold values from -6 to 6
- expert_gate_weight: bfloat16 [8, 2048, 2048], P('sp', None, 'tp'), may hold values from -0.125 to 0.125
- expert_up_weight: bfloat16 [8, 2048, 2048], P('sp', None, 'tp'), may hold values from -0.125 to 0.125
- expert_down_weight: bfloat16 [8, 2048, 2048], P('sp', 'tp'), may hold values from -0.125 to 0.125
Outputs:
- grad_queries: float32 [512, 1024], P('tp', 'sp')
- grad_keys: float32 [512, 1024], P('tp', 'sp')
- grad_values: float32 [1024, 1024], P('tp', 'sp')
- grad_logit: float32 [512, 1024], P('tp', 'sp')
- grad_out_proj: float32 [2048, 1024], P('sp', 'tp')
- grad_gate: bfloat16 [8, 2048, 2048], P('sp', None, 'tp')
- grad_up: bfloat16 [8, 2048, 2048], P('sp', None, 'tp')
- grad_down: bfloat16 [8, 2048, 2048], P('sp', 'tp')
The draws below stay inside these ranges and needn't reach their ends.
Inputs may be any that keep to these rules, and one draw needn't show every extreme that they name: `chosen_expert_index`: each position names two different experts; in the rows of one device no expert is named more than 48 times. `channel_decay_speed`: positive. `extra_log_decay`: zero or negative.
All inputs are finite; a program needn't handle non-finite values.
Results may differ from the reference program's by a relative error of at most 0.023.
Values may be sent and summed in bfloat16 or wider, within the bound.
A program may use at most 64 MiB of HBM per device.

```python
import math
import jax
import jax.numpy as jnp
import numpy as np
from jax import lax

D = 2048
HEADS = 16
KEY_DIM = 32
VAL_DIM = 64
EXPERT_UNITS = 2048
TOK_DEV = 128
SPAN = 64
SEQUENCE_LENGTH = 1024
EXPERTS = 8
CAP = 48
KEY_CHANNELS = 512
VCH = 1024
N_SP = 8
N_TP = 4


def draw_channel_decay_speed(key, part):
    key_pick, key_spread = jax.random.split(jax.random.fold_in(key, 11))
    slow_share = 0.5
    is_slow = jax.random.uniform(key_pick, (KEY_CHANNELS,), jnp.float32) < slow_share
    spread = jax.random.uniform(key_spread, (KEY_CHANNELS,), jnp.float32)
    slow_rate = jnp.exp(jnp.log(0.2) + spread * (jnp.log(1.0) - jnp.log(0.2))) / SEQUENCE_LENGTH
    fast_rate = jnp.exp(jnp.log(0.02) + spread * (jnp.log(0.06) - jnp.log(0.02)))
    return jnp.where(is_slow, slow_rate, fast_rate).astype(jnp.float32)


def draw_decay_preactivation(key, part):
    key_noise, key_level = jax.random.split(jax.random.fold_in(key, 23))
    noise = jnp.clip(jax.random.normal(key_noise, (KEY_CHANNELS, SEQUENCE_LENGTH), jnp.float32), -4.0, 4.0)
    level = jax.random.uniform(key_level, (SEQUENCE_LENGTH // TOK_DEV,), jnp.float32, -1.5, 1.5)
    return (noise + jnp.repeat(level, TOK_DEV)[None, :]).astype(jnp.bfloat16)


def draw_extra_log_decay(key, part):
    key_channel_index, key_channel_count = jax.random.split(jax.random.fold_in(key, 37))
    jump_location = jax.random.randint(key_channel_index, (KEY_CHANNELS, 3), 0, SEQUENCE_LENGTH)
    jump_magnitude = jax.random.uniform(key_channel_count, (KEY_CHANNELS, 3), jnp.float32, jnp.log(0.6), jnp.log(0.8))
    jump_hit_mask = jnp.arange(SEQUENCE_LENGTH, dtype=jnp.int32)[None, None, :] == jump_location[:, :, None]
    return jnp.sum(jnp.where(jump_hit_mask, jump_magnitude[:, :, None], 0.0), axis=1).astype(jnp.float32)


def raised(values, key, source, target, shards_of, factor):
    def block_of(axis_at):
        return (jnp.arange(values.shape[axis_at]) // (values.shape[axis_at] // shards_of)).reshape((-1,) + (1,) * (values.ndim - 1 - axis_at))

    one_side = jax.random.permutation(key, shards_of)[block_of(target)]
    second = (block_of(target) + shards_of // 2) % shards_of
    return jnp.where((block_of(source) == one_side) | (block_of(source) == second), factor * values, values)


def levels(key, dims, cuts, smallest, top_value):
    level = 1.0
    for axis_at, shards_of in cuts:
        draws = jax.random.uniform(jax.random.fold_in(jax.random.fold_in(key, 6), axis_at), (shards_of,), jnp.float32, smallest / len(cuts), top_value / len(cuts))
        level = level * jnp.repeat(jnp.exp(draws), dims[axis_at] // shards_of).reshape((-1,) + (1,) * (len(dims) - 1 - axis_at))
    return level


def assign_block(key, own, number, rows, number_of, top, most, slope):
    order = jax.random.permutation(key, number_of)
    crowded, ordinary = load_shares(number_of, rows * top, most, slope, True), load_shares(number_of, rows * top, most, slope, False)
    places = jnp.arange(number_of)

    def named(sizes, offset_by):
        used = int((sizes > 0).sum())
        fixed = max(1, used // 4)
        moved = fixed + (places - fixed + offset_by * (used - fixed)) % max(1, number_of - fixed)
        return jnp.zeros((number_of,), jnp.int32).at[order[jnp.where(places < fixed, places, moved)]].set(jnp.asarray(sizes, jnp.int32))

    sizes = jnp.where(number % 4 == 0, named(crowded, number // 4), named(ordinary, number - number // 4 - 1))
    mixed = jax.random.permutation(jax.random.fold_in(own, 3), number_of)
    donor, receiver = mixed[0:number_of // 2 * 2:2], mixed[1:number_of // 2 * 2:2]
    margin = jnp.minimum(sizes[donor] - 1, most - sizes[receiver]) // 2
    margin = jnp.where((donor == order[0]) | (receiver == order[0]) | (sizes[receiver] == 0), 0, jnp.maximum(margin, 0))
    moved = jax.random.randint(jax.random.fold_in(own, 4), (number_of // 2,), 0, 1 << 20) % (margin + 1)
    sizes = sizes.at[donor].add(-moved).at[receiver].add(moved)
    items = jnp.searchsorted(jnp.cumsum(sizes), jnp.arange(rows * top), side="right").astype(jnp.int32)
    table = items.reshape(top, rows).T
    table = table[jax.random.permutation(jax.random.fold_in(own, 1), rows)]
    offset_by = jax.random.randint(jax.random.fold_in(own, 2), (rows, 1), 0, top)
    return jnp.take_along_axis(table, (jnp.arange(top)[None, :] + offset_by) % top, axis=1)


def load_shares(count, total, bound, lean, full):
    portions = [(1 << 20) // math.isqrt(rank ** lean) + 1 for rank in range(1, count + 1)]
    largest = bound if full else min(bound, max(-(-total // count), total * portions[0] // sum(portions)))
    least = 1 if total - largest >= count - 1 else 0
    holding, rest = [largest] + [least] * (count - 1), total - largest - least * (count - 1)
    while rest > 0:
        free = [i for i in range(1, count) if holding[i] < largest] or [i for i in range(1, count) if holding[i] < bound]
        mass, left = sum([portions[i] for i in free]), rest
        for i in free:
            extra = min(bound - holding[i], max(1, left * portions[i] // mass), rest)
            holding[i] = holding[i] + extra
            rest = rest - extra
    return np.array(holding)


def normal_values(rng, shape, deviation, limit, shards=(), kind=jnp.bfloat16):
    factor_of = levels(rng, shape, shards, -0.22, 0.18) if shards else 1.0
    drawn = jax.random.normal(rng, shape, jnp.float32) * deviation * factor_of
    return jnp.minimum(jnp.maximum(drawn, -limit), limit).astype(kind)


def bell_draw_with(rng, extent, width, bound, cuts, heavy, kind=jnp.bfloat16):
    entries = width * jax.random.normal(rng, extent, jnp.float32)
    if cuts:
        entries = entries * levels(rng, extent, cuts, -0.22, 0.18)
    return jnp.clip(raised(entries, jax.random.fold_in(rng, 3), *heavy), -bound, bound).astype(kind)


def setup_inputs(seed: int = 0) -> dict:
    keys = jax.random.split(jax.random.key(seed), 15)
    queries = normal_values(keys[0], (KEY_CHANNELS, SEQUENCE_LENGTH), 1.0, 6.0, ((0, 4), (1, 8)))
    input_key_matrix = normal_values(keys[1], (KEY_CHANNELS, SEQUENCE_LENGTH), 1.0, 6.0, ((0, 4), (1, 8)))
    input_value_matrix = normal_values(keys[2], (VCH, SEQUENCE_LENGTH), 1.0, 6.0, ((0, 4), (1, 8)))
    decay_preactivation = draw_decay_preactivation(jax.random.fold_in(keys[14], 71), 0)
    extra_log_decay = draw_extra_log_decay(jax.random.fold_in(keys[14], 71), 0)
    channel_decay_speed = draw_channel_decay_speed(jax.random.fold_in(keys[14], 71), 0)
    output_weight_matrix = normal_values(keys[6], (D, VCH), VCH ** -0.5, 0.1875, ((1, 4),))
    stored_expert_rows = normal_values(keys[7], (SEQUENCE_LENGTH, D), 1.0, 6.0, ((0, 8), (1, 4)))
    chosen_expert_index_keys = jax.random.split(jax.random.fold_in(keys[8], 1), SEQUENCE_LENGTH // TOK_DEV)
    chosen_expert_index_turns = jax.random.permutation(jax.random.fold_in(keys[8], 3), SEQUENCE_LENGTH // TOK_DEV)
    chosen_expert_index = jax.vmap(lambda own, number: assign_block(jax.random.fold_in(keys[8], 2), own, number, TOK_DEV, EXPERTS, 2, CAP, 1))(chosen_expert_index_keys, chosen_expert_index_turns).reshape((SEQUENCE_LENGTH, 2))
    expert_combine_weight = jnp.clip(0.2 + 0.8 * jax.random.uniform(keys[9], (SEQUENCE_LENGTH, 2), jnp.float32) ** levels(keys[9], (SEQUENCE_LENGTH, 2), ((0, 8),), -0.2, 0.2), 0.2, 1.0)
    cotangent = bell_draw_with(keys[10], (SEQUENCE_LENGTH, D), 1.0, 6.0, ((0, 8), (1, 4)), (0, 1, 8, 2.0))
    expert_gate_weight = normal_values(keys[11], (EXPERTS, D, EXPERT_UNITS), D ** -0.5, 0.125, ((0, 8), (2, 4)))
    expert_up_weight = normal_values(keys[12], (EXPERTS, D, EXPERT_UNITS), D ** -0.5, 0.125, ((0, 8), (2, 4)))
    expert_down_weight = normal_values(keys[13], (EXPERTS, EXPERT_UNITS, D), EXPERT_UNITS ** -0.5, 0.125, ((0, 8), (1, 4)))
    return dict(queries=queries, input_key_matrix=input_key_matrix, input_value_matrix=input_value_matrix, decay_preactivation=decay_preactivation, extra_log_decay=extra_log_decay, channel_decay_speed=channel_decay_speed, output_weight_matrix=output_weight_matrix, stored_expert_rows=stored_expert_rows, chosen_expert_index=chosen_expert_index, expert_combine_weight=expert_combine_weight, cotangent=cotangent, expert_gate_weight=expert_gate_weight, expert_up_weight=expert_up_weight, expert_down_weight=expert_down_weight)


def combine_steps(state, pair):
    factor, addend = pair
    return (factor * state + addend, state)

def head_forward(scaled, key_feats, val_feats, decay_logarithm):
    blocks = decay_logarithm.shape[1] // SPAN

    def split_blocks(array):
        return array.reshape(array.shape[0], blocks, SPAN).transpose(1, 0, 2)
    block_q = split_blocks(scaled)
    block_k = split_blocks(key_feats)
    block_v = split_blocks(val_feats)
    cumulative = jnp.cumsum(split_blocks(decay_logarithm), axis=2)
    total_log = cumulative[:, :, -1:]
    lower_mask = lax.broadcasted_iota(jnp.int32, (SPAN, SPAN), 0) >= lax.broadcasted_iota(jnp.int32, (SPAN, SPAN), 1)
    log_gap = cumulative[:, :, :, None] - cumulative[:, :, None, :]
    weight = jnp.exp(jnp.where(lower_mask, log_gap, -log_gap))
    scores = jnp.einsum('bct,bcs,bcts->bts', block_q, block_k, weight)
    inner_part = jnp.einsum('bts,bvs->bvt', scores, block_v)
    factor = jnp.exp(total_log)
    fwd_sum = jnp.einsum('bcs,bvs->bcv', block_k * jnp.exp(total_log - cumulative), block_v)
    bwd_sum = jnp.einsum('bcs,bvs->bcv', block_k * jnp.exp(cumulative), block_v)
    start_state = jnp.zeros((key_feats.shape[0], val_feats.shape[0]), jnp.float32)
    _, fwd_in = lax.scan(combine_steps, start_state, (factor, fwd_sum))
    _, bwd_in = lax.scan(combine_steps, start_state, (factor, bwd_sum), reverse=True)
    carried = jnp.einsum('bct,bcv->bvt', block_q * jnp.exp(cumulative), fwd_in)
    carried = carried + jnp.einsum('bct,bcv->bvt', block_q * jnp.exp(total_log - cumulative), bwd_in)
    output = inner_part + carried
    return output.transpose(1, 0, 2).reshape(val_feats.shape[0], -1)

def head_mix(query_f, key_feats, val_feats, decay_logarithm):
    return head_forward(query_f * KEY_DIM ** (-0.5), key_feats, val_feats, decay_logarithm)

def head_apply(packed):
    return head_mix(packed[0], packed[1], packed[2], packed[3])

def head_grads(packed):
    _, pull_back = jax.vjp(head_mix, packed[0], packed[1], packed[2], packed[3])
    return pull_back(packed[4])

def expert_grads(packed):
    slot_table, gate_local, up_local, down_local, inputs_pad, grads_pad = packed
    rows_x = inputs_pad[slot_table // 2]
    rows_dy = grads_pad[slot_table]
    gate_pre = jnp.dot(rows_x, gate_local, preferred_element_type=jnp.float32)
    up_pre = jnp.dot(rows_x, up_local, preferred_element_type=jnp.float32)
    gate_sig = jax.nn.sigmoid(gate_pre)
    gate_act = gate_pre * gate_sig
    hidden = (gate_act * up_pre).astype(jnp.bfloat16)
    grad_down = jnp.dot(hidden.T, rows_dy, preferred_element_type=jnp.float32).astype(jnp.bfloat16)
    grad_hidden = jnp.dot(rows_dy, down_local.T, preferred_element_type=jnp.float32)
    grad_gate_pre = (grad_hidden * up_pre * gate_sig * (1.0 + gate_pre * (1.0 - gate_sig))).astype(jnp.bfloat16)
    grad_up_pre = (grad_hidden * gate_act).astype(jnp.bfloat16)
    grad_gate = jnp.dot(rows_x.T, grad_gate_pre, preferred_element_type=jnp.float32).astype(jnp.bfloat16)
    grad_up = jnp.dot(rows_x.T, grad_up_pre, preferred_element_type=jnp.float32).astype(jnp.bfloat16)
    row_count = rows_x.shape[0]
    group_width = EXPERT_UNITS // N_TP
    gate_groups = grad_gate_pre.astype(jnp.float32).reshape(row_count, N_TP, group_width)
    up_groups = grad_up_pre.astype(jnp.float32).reshape(row_count, N_TP, group_width)
    gate_weights = gate_local.astype(jnp.float32).reshape(D, N_TP, group_width)
    up_weights = up_local.astype(jnp.float32).reshape(D, N_TP, group_width)
    partial_value = jnp.einsum('rjh,djh->jrd', gate_groups, gate_weights) + jnp.einsum('rjh,djh->jrd', up_groups, up_weights)
    partial_value = partial_value.astype(jnp.bfloat16).astype(jnp.float32)
    slot_grads = lax.optimization_barrier(jnp.sum(partial_value, axis=0)).astype(jnp.bfloat16)
    return (grad_gate, grad_up, grad_down, slot_grads)

def reference(queries, input_key_matrix, input_value_matrix, decay_preactivation, extra_log_decay, channel_decay_speed, output_weight_matrix, stored_expert_rows, chosen_expert_index, expert_combine_weight, cotangent, expert_gate_weight, expert_up_weight, expert_down_weight):
    preactivation_single = decay_preactivation.astype(jnp.float32)
    decay_logarithm = channel_decay_speed[:, None] * jax.nn.log_sigmoid(preactivation_single) + extra_log_decay
    query_heads = queries.astype(jnp.float32).reshape(HEADS, KEY_DIM, SEQUENCE_LENGTH)
    key_heads = input_key_matrix.astype(jnp.float32).reshape(HEADS, KEY_DIM, SEQUENCE_LENGTH)
    value_heads = input_value_matrix.astype(jnp.float32).reshape(HEADS, VAL_DIM, SEQUENCE_LENGTH)
    decay_heads = decay_logarithm.reshape(HEADS, KEY_DIM, SEQUENCE_LENGTH)
    mixed = lax.map(head_apply, (query_heads, key_heads, value_heads, decay_heads))
    inv_rms = lax.rsqrt(lax.optimization_barrier(jnp.mean(mixed * mixed, axis=1, keepdims=True)) + 1e-06)
    normed = mixed * inv_rms
    mix_rows = normed.astype(jnp.bfloat16).reshape(VCH, SEQUENCE_LENGTH)
    block_ids = chosen_expert_index.reshape(N_SP, 2 * TOK_DEV)
    onehot = (block_ids[:, :, None] == jnp.arange(EXPERTS, dtype=jnp.int32)[None, None, :]).astype(jnp.int32)
    slot_rank = lax.optimization_barrier(jnp.sum((jnp.cumsum(onehot, axis=1) - onehot) * onehot, axis=2))
    source = jnp.arange(N_SP, dtype=jnp.int32)[:, None]
    flat_slot = (block_ids * (N_SP * CAP) + source * CAP + slot_rank).reshape(-1)
    slot_table = jnp.full((EXPERTS * N_SP * CAP,), 2 * SEQUENCE_LENGTH, jnp.int32)
    slot_table = slot_table.at[flat_slot].set(jnp.arange(2 * SEQUENCE_LENGTH, dtype=jnp.int32))
    zero_row = jnp.zeros((1, D), jnp.bfloat16)
    inputs_pad = jnp.concatenate([stored_expert_rows, zero_row], axis=0)
    weighted = (expert_combine_weight.reshape(-1, 1) * jnp.repeat(cotangent, 2, axis=0).astype(jnp.float32)).astype(jnp.bfloat16)
    grads_pad = jnp.concatenate([weighted, zero_row], axis=0)

    def per_expert(packed):
        return expert_grads((packed[0], packed[1], packed[2], packed[3], inputs_pad, grads_pad))
    grad_gate, grad_up, grad_down, slot_grads = lax.map(per_expert, (slot_table.reshape(EXPERTS, N_SP * CAP), expert_gate_weight, expert_up_weight, expert_down_weight))
    picked = slot_grads.reshape(EXPERTS * N_SP * CAP, D)[flat_slot].astype(jnp.float32).reshape(SEQUENCE_LENGTH, 2, D)
    token_grads = (cotangent.astype(jnp.float32) + picked[:, 0] + picked[:, 1]).astype(jnp.bfloat16)
    grad_out_proj = jnp.dot(token_grads.T, mix_rows.T, preferred_element_type=jnp.float32)
    grad_normed = jnp.dot(output_weight_matrix.T, token_grads.T, preferred_element_type=jnp.float32).reshape(HEADS, VAL_DIM, SEQUENCE_LENGTH)
    grad_mixed = inv_rms * (grad_normed - normed * lax.optimization_barrier(jnp.mean(grad_normed * normed, axis=1, keepdims=True)))
    grad_q, grad_k, grad_v, grad_decay = lax.map(head_grads, (query_heads, key_heads, value_heads, decay_heads, grad_mixed))
    grad_logit = grad_decay.reshape(KEY_CHANNELS, SEQUENCE_LENGTH) * channel_decay_speed[:, None] * jax.nn.sigmoid(-preactivation_single)
    return (grad_q.reshape(KEY_CHANNELS, SEQUENCE_LENGTH), grad_k.reshape(KEY_CHANNELS, SEQUENCE_LENGTH), grad_v.reshape(VCH, SEQUENCE_LENGTH), grad_logit, grad_out_proj, grad_gate, grad_up, grad_down)
```

```python
import functools

import jax
import jax.numpy as jnp
from jax import lax
from jax.experimental import pallas as pl
from jax.experimental.pallas import tpu as pltpu
from jax.sharding import PartitionSpec as P

KEY_DIM = 32
VAL_DIM = 64
CORES = 2
BF16 = jnp.bfloat16
F32 = jnp.float32
MESH = pl.DeviceIdType.MESH
VMEM_LIMIT = 60 * 1024 * 1024
TN = ((0,), (0,))
NN = ((1,), (0,))
NT = ((1,), (1,))


def dot(a, b, contract):
    return lax.dot_general(a.astype(BF16), b.astype(BF16), (contract, ((), ())),
                           preferred_element_type=F32)


def exact_dot(a, b):
    return lax.dot_general(a, b, (((1,), (0,)), ((), ())), precision=lax.Precision.HIGHEST,
                           preferred_element_type=F32)


def triangle(length, test):
    rows = lax.broadcasted_iota(jnp.int32, (length, length), 0)
    cols = lax.broadcasted_iota(jnp.int32, (length, length), 1)
    return test(rows, cols)


def loop(count, step):
    lax.fori_loop(0, count, lambda i, _: (step(i), 0)[1], 0)


class Peers:
    def __init__(self, n, m):
        self.n, self.m, self.chips = n, m, m // CORES
        self.me, self.tp = lax.axis_index("sp"), lax.axis_index("tp")
        self.chip, self.core = lax.div(self.tp, CORES), lax.rem(self.tp, CORES)
        self.mate = self.chip * CORES + (1 - self.core)

    def to(self, d):
        return lax.rem(self.me + d, self.n)

    def source(self, d):
        return lax.rem(self.me - d + self.n, self.n)

    def to_chip(self, d):
        return lax.rem(self.chip + d, self.chips) * CORES + self.core

    def from_chip(self, d):
        return lax.rem(self.chip - d + self.chips, self.chips) * CORES + self.core

    def mate_from_chip(self, d):
        return lax.rem(self.chip - d + self.chips, self.chips) * CORES + (1 - self.core)

    def greet(self):
        barrier = pltpu.get_barrier_semaphore()

        def signal(device):
            pl.semaphore_signal(barrier, inc=1, device_id=device, device_id_type=MESH)

        loop(self.n - 1, lambda i: signal({"sp": self.to(i + 1)}))
        for d in range(1, self.chips):
            signal({"tp": self.to_chip(d)})
        signal({"tp": self.mate})

    def met(self):
        pl.semaphore_wait(pltpu.get_barrier_semaphore(), self.n - 1 + self.chips)


def copy_to(src, dst, send, recv, device):
    return pltpu.make_async_remote_copy(src_ref=src, dst_ref=dst, send_sem=send, recv_sem=recv,
                                        device_id=device, device_id_type=MESH)


def own_heads(stacked, width):
    heads = stacked.shape[0] // width
    head = lax.broadcasted_iota(jnp.int32, (width, stacked.shape[1]), 1) // KEY_DIM
    out = jnp.zeros((width, stacked.shape[1]), F32)
    for h in range(heads):
        out = jnp.where(head == h, stacked[h * width:(h + 1) * width], out)
    return out


def spread_heads(state, heads):
    head = lax.broadcasted_iota(jnp.int32, state.shape, 1) // KEY_DIM
    return jnp.concatenate([jnp.where(head == h, state, 0.0) for h in range(heads)], axis=0)


def as_row(column):
    length = column.shape[0]
    diagonal = triangle(length, lambda a, b: a == b)
    return jnp.sum(jnp.where(diagonal, column, 0.0), axis=0, keepdims=True)


def as_column(row):
    length = row.shape[1]
    diagonal = triangle(length, lambda a, b: a == b)
    return jnp.sum(jnp.where(diagonal, row, 0.0), axis=1, keepdims=True)


def carry(n, me, state_of, factor_of):
    shape = state_of(0).shape
    before, after = jnp.zeros(shape, F32), jnp.zeros(shape, F32)
    for i in range(n):
        before = jnp.where(i < me, before * factor_of(i) + state_of(i), before)
    for i in reversed(range(n)):
        after = jnp.where(i > me, after * factor_of(i) + state_of(i), after)
    return before, after


def dispatch_kernel(n, m, cap, q_ref, k_ref, v_ref, pre_ref, extra_ref, speed_ref, x_ref, cot_ref,
                    pick_ref, comb_ref, gate_any, up_any, down_any,
                    rows_ref, hidden_ref, ggp_ref, gup_ref, place_ref, st_ref, cum_ref,
                    normed_ref, inv_ref, mix_ref, carried_ref, last_ref,
                    send_ref, sbuf, sin, lbuf, inner_ref, gate_v, up_v, down_v, gp_ref, up_ref,
                    zs, zr, ys, yr, ps, pr, ss, sr, ws):
    at = Peers(n, m)
    me = at.me
    tok, channels = q_ref.shape[1], q_ref.shape[0]
    width = x_ref.shape[1]
    heads = channels // KEY_DIM
    slots = n * cap
    at.greet()
    loads = [pltpu.make_async_copy(src, dst, ws.at[i])
             for i, (src, dst) in enumerate(((gate_any, gate_v), (up_any, up_v),
                                             (down_any, down_v)))]
    for load in loads:
        load.start()

    expert = lax.broadcasted_iota(jnp.int32, (n, tok), 0)
    picks = [pick_ref[i:i + 1, :] == expert for i in range(2)]
    named = (picks[0] | picks[1]).astype(F32)
    counts = dot(named, triangle(tok, lambda a, b: a < b).astype(F32), NN)
    slot = lax.broadcasted_iota(jnp.int32, (slots, tok), 0)
    places = []
    for i in range(2):
        rank = jnp.sum(jnp.where(picks[i], counts, 0.0), axis=0, keepdims=True)
        places.append(slot == pick_ref[i:i + 1, :] * cap + rank.astype(jnp.int32))
    place = (places[0] | places[1]).astype(BF16)
    place_ref[...] = place
    weight = jnp.sum(jnp.where(places[0], comb_ref[0:1, :], 0.0)
                     + jnp.where(places[1], comb_ref[1:2, :], 0.0), axis=1, keepdims=True)
    send_ref[0] = dot(place, x_ref[...], NN).astype(BF16)
    send_ref[1] = (weight * dot(place, cot_ref[...], NN)).astype(BF16)

    def rows(p):
        return pl.ds(pl.multiple_of(p * cap, 16), cap)

    for t in range(2):
        rows_ref[t, at.tp, rows(me), :] = send_ref[t, rows(me), :]

    def out_row(t, d):
        p = at.to(d)
        return copy_to(send_ref.at[t, rows(p)], rows_ref.at[t, at.tp, rows(me)],
                       zs.at[t, d], zr.at[t, d], {"sp": p})

    def in_row(t, d):
        p = at.source(d)
        here = rows_ref.at[t, at.tp, rows(p)]
        return copy_to(here, here, zs.at[t, d], zr.at[t, d], {"sp": p})

    def across(t, d, dy):
        here = rows_ref.at[t, at.tp, rows(at.source(d))]
        return copy_to(here, here, ys.at[t, dy, d], yr.at[t, dy, d], {"tp": at.to_chip(dy)})

    def across_in(t, d, dy):
        here = rows_ref.at[t, at.from_chip(dy), rows(at.source(d))]
        return copy_to(here, here, ys.at[t, dy, d], yr.at[t, dy, d], {"tp": at.from_chip(dy)})

    def relay(t, d, dy):
        here = rows_ref.at[t, at.from_chip(dy), rows(at.source(d))]
        return copy_to(here, here, ps.at[t, dy, d], pr.at[t, dy, d], {"tp": at.mate})

    def relay_in(t, d, dy):
        here = rows_ref.at[t, at.mate_from_chip(dy), rows(at.source(d))]
        return copy_to(here, here, ps.at[t, dy, d], pr.at[t, dy, d], {"tp": at.mate})

    def pass_on(t, d):
        @pl.when(d > 0)
        def _():
            in_row(t, d).wait_recv()
        for dy in range(1, at.chips):
            across(t, d, dy).start()
        relay(t, d, 0).start()

    def pass_mate(t, d):
        for dy in range(1, at.chips):
            across_in(t, d, dy).wait_recv()
            relay(t, d, dy).start()

    def gathered(t, d):
        for dy in range(at.chips):
            relay_in(t, d, dy).wait_recv()

    at.met()
    for t in range(2):
        loop(n - 1, lambda i, t=t: out_row(t, i + 1).start())

    pre = pre_ref[...].astype(F32)
    log_sig = jnp.minimum(pre, 0.0) - jnp.log1p(jnp.exp(-jnp.abs(pre)))
    decays = as_column(speed_ref[...]) * log_sig + extra_ref[...]
    cum_ref[...] = exact_dot(decays, triangle(tok, lambda a, b: a <= b).astype(F32))

    per_head = -(-n // heads)

    def head(h):
        keys = pl.ds(pl.multiple_of(h * KEY_DIM, KEY_DIM), KEY_DIM)
        values = pl.ds(pl.multiple_of(h * VAL_DIM, VAL_DIM), VAL_DIM)
        q = q_ref[keys, :].astype(F32) * KEY_DIM ** (-0.5)
        cum = cum_ref[keys, :]
        cum_t = cum.T
        k_t = k_ref[keys, :].astype(F32).T
        total = jnp.zeros((tok, tok), F32)
        for c in range(KEY_DIM):
            decay = jnp.exp(-jnp.abs(cum_t[:, c:c + 1] - cum[c:c + 1, :]))
            total = total + (k_t[:, c:c + 1] * q[c:c + 1, :]) * decay
        scores = total.astype(BF16)
        st_ref[pl.ds(pl.multiple_of(h * tok, tok), tok), :] = scores
        inner_ref[values, :] = dot(v_ref[values, :], scores, NN)

        def forward(i):
            @pl.when(h * per_head + i < n)
            def _():
                pass_on(0, h * per_head + i)
        loop(per_head, forward)

    loop(heads, head)

    cum = cum_ref[...]
    last = cum[:, tok - 1:tok]
    k = k_ref[...].astype(F32)
    sbuf[0] = own_heads(dot(v_ref[...], k * jnp.exp(last - cum), NT), VAL_DIM).astype(BF16)
    sbuf[1] = own_heads(dot(v_ref[...], k * jnp.exp(cum), NT), VAL_DIM).astype(BF16)
    lbuf[...] = jnp.broadcast_to(as_row(last), lbuf.shape)
    sin[me] = jnp.zeros(sin.shape[1:], BF16)
    last_ref[me] = jnp.zeros(last_ref.shape[1:], F32)

    def out_state(d):
        p = at.to(d)
        return (copy_to(sbuf.at[jnp.where(p > me, 0, 1)], sin.at[me], ss.at[0, d], sr.at[0, d],
                        {"sp": p}),
                copy_to(lbuf, last_ref.at[me], ss.at[1, d], sr.at[1, d], {"sp": p}))

    def in_state(d):
        p = at.source(d)
        return (copy_to(sbuf.at[0], sin.at[p], ss.at[0, d], sr.at[0, d], {"sp": p}),
                copy_to(lbuf, last_ref.at[p], ss.at[1, d], sr.at[1, d], {"sp": p}))

    loop(n - 1, lambda i: [copy.start() for copy in out_state(i + 1)] and None)

    half = n // 2
    loop(n, lambda d: pass_mate(0, d))
    loop(half, lambda d: pass_on(1, d))
    loop(n, lambda d: gathered(0, d))

    def columns_of(weights, t):
        total = None
        for j in range(m):
            part = dot(rows_ref[t, j], weights[j * width:(j + 1) * width, :], NN)
            total = part if total is None else total + part
        return total

    loads[0].wait()
    gp_ref[...] = columns_of(gate_v, 0)
    loop(n - half, lambda d: pass_on(1, d + half))
    loads[1].wait()
    up_ref[...] = columns_of(up_v, 0)
    loop(n, lambda d: pass_mate(1, d))

    loop(n - 1, lambda i: [copy.wait_recv() for copy in in_state(i + 1)] and None)
    before, after = carry(n, me, lambda i: sin[i].astype(F32),
                          lambda i: jnp.exp(last_ref[i, 0:1, :]))
    carried_ref[0] = before
    carried_ref[1] = after
    q = q_ref[...].astype(F32) * KEY_DIM ** (-0.5)
    mixed = inner_ref[...] + dot(spread_heads(before, heads), q * jnp.exp(cum), NN)
    mixed = mixed + dot(spread_heads(after, heads), q * jnp.exp(last - cum), NN)
    for h in range(heads):
        part = mixed[h * VAL_DIM:(h + 1) * VAL_DIM]
        inv = lax.rsqrt(jnp.mean(part * part, axis=0, keepdims=True) + 1e-06)
        normed = part * inv
        normed_ref[h * VAL_DIM:(h + 1) * VAL_DIM, :] = normed
        mix_ref[h * VAL_DIM:(h + 1) * VAL_DIM, :] = normed.astype(BF16)
        inv_ref[h * 8:(h + 1) * 8, :] = jnp.broadcast_to(inv, (8, tok))

    loop(n, lambda d: gathered(1, d))
    loads[2].wait()
    grad_hidden = None
    for j in range(m):
        part = dot(rows_ref[1, j], down_v[:, j * width:(j + 1) * width], NT)
        grad_hidden = part if grad_hidden is None else grad_hidden + part
    gate_pre, up_pre = gp_ref[...], up_ref[...]
    gate_sig = jax.nn.sigmoid(gate_pre)
    gate_act = gate_pre * gate_sig
    hidden_ref[...] = (gate_act * up_pre).astype(BF16)
    ggp_ref[...] = (grad_hidden * up_pre * gate_sig
                    * (1.0 + gate_pre * (1.0 - gate_sig))).astype(BF16)
    gup_ref[...] = (grad_hidden * gate_act).astype(BF16)

    def drain(i):
        for copy in out_state(i + 1):
            copy.wait_send()
        for t in range(2):
            out_row(t, i + 1).wait_send()
    loop(n - 1, drain)

    def drain_passed(d):
        for t in range(2):
            for dy in range(1, at.chips):
                across(t, d, dy).wait_send()
            for dy in range(at.chips):
                relay(t, d, dy).wait_send()
    loop(n, drain_passed)


def vmem_specs(count):
    return [pl.BlockSpec(memory_space=pltpu.VMEM)] * count


def dispatch(n, m, cap, q, k, v, pre, extra, speed, x, cot, picks, comb, gate, up, down):
    channels, tok = q.shape
    values = v.shape[0]
    heads = channels // KEY_DIM
    slots, width, units = n * cap, x.shape[1], gate.shape[1]
    chips = m // CORES
    dma = pltpu.SemaphoreType.DMA
    outs = [((2, m, slots, width), BF16), ((slots, units), BF16), ((slots, units), BF16),
            ((slots, units), BF16), ((slots, tok), BF16), ((heads * tok, tok), BF16),
            ((channels, tok), F32), ((values, tok), F32), ((heads * 8, tok), F32),
            ((values, tok), BF16), ((2, VAL_DIM, channels), F32), ((n, 8, channels), F32)]
    return pl.pallas_call(
        functools.partial(dispatch_kernel, n, m, cap),
        in_specs=vmem_specs(10) + [pl.BlockSpec(memory_space=pl.ANY)] * 3,
        out_specs=vmem_specs(len(outs)),
        out_shape=[jax.ShapeDtypeStruct(shape, dtype) for shape, dtype in outs],
        scratch_shapes=[
            pltpu.VMEM((2, slots, width), BF16), pltpu.VMEM((2, VAL_DIM, channels), BF16),
            pltpu.VMEM((n, VAL_DIM, channels), BF16), pltpu.VMEM((8, channels), F32),
            pltpu.VMEM((values, tok), F32),
            pltpu.VMEM(gate.shape, BF16), pltpu.VMEM(up.shape, BF16), pltpu.VMEM(down.shape, BF16),
            pltpu.VMEM((slots, units), F32), pltpu.VMEM((slots, units), F32),
            dma((2, n)), dma((2, n)), dma((2, chips, n)), dma((2, chips, n)),
            dma((2, chips, n)), dma((2, chips, n)), dma((2, n)), dma((2, n)), dma((3,)),
        ],
        compiler_params=pltpu.CompilerParams(collective_id=0, has_side_effects=True,
                                             vmem_limit_bytes=VMEM_LIMIT),
        name="dispatch",
    )(q, k, v, pre, extra, speed, x, cot, picks, comb, gate, up, down)


def source_kernel(gn_ref, normed_ref, inv_ref, q_ref, cum_ref, dm_ref, fwd_ref, bwd_ref):
    length = q_ref.shape[1]
    normed = normed_ref[...]
    gn = gn_ref[...]
    dm = inv_ref[0:1, :] * (gn - normed * jnp.mean(gn * normed, axis=0, keepdims=True))
    dm_ref[...] = dm
    q = q_ref[...].astype(F32) * KEY_DIM ** (-0.5)
    cum = cum_ref[...]
    last = cum[:, length - 1:length]
    fwd = dot(q * jnp.exp(cum), dm, ((1,), (1,)))
    bwd = dot(q * jnp.exp(last - cum), dm, ((1,), (1,)))
    pad = jnp.zeros_like(fwd)
    fwd_ref[...] = jnp.concatenate([fwd, pad], axis=1).astype(BF16)
    bwd_ref[...] = jnp.concatenate([bwd, pad], axis=1).astype(BF16)


def inner_kernel(dm_ref, q_ref, k_ref, v_ref, cum_ref, st_ref, carried_ref,
                 dq_ref, dk_ref, dv_ref, dc_ref, dt_ref):
    length = q_ref.shape[1]
    dm = dm_ref[...]
    q = q_ref[...].astype(F32) * KEY_DIM ** (-0.5)
    k = k_ref[...].astype(F32)
    v = v_ref[...]
    cum = cum_ref[...]
    by_query = dot(dm, v, ((0,), (0,)))
    by_key = dot(v, dm, ((0,), (0,)))
    sign = jnp.where(triangle(length, lambda a, b: a > b), 1.0,
                     jnp.where(triangle(length, lambda a, b: a < b), -1.0, 0.0)).astype(F32)
    by_query_signed = by_query * sign
    by_key_signed = by_key * -sign
    cum_t, q_t, k_t = cum.T, q.T, k.T
    dq, dk, dq_signed, dk_signed = [], [], [], []
    for c in range(KEY_DIM):
        weight = jnp.exp(-jnp.abs(cum_t[:, c:c + 1] - cum[c:c + 1, :]))
        with_q = weight * q_t[:, c:c + 1]
        with_k = weight * k_t[:, c:c + 1]
        dk.append(jnp.sum(by_query * with_q, axis=0, keepdims=True))
        dk_signed.append(jnp.sum(by_query_signed * with_q, axis=0, keepdims=True))
        dq.append(jnp.sum(by_key * with_k, axis=0, keepdims=True))
        dq_signed.append(jnp.sum(by_key_signed * with_k, axis=0, keepdims=True))
    join = lambda rows: jnp.concatenate(rows, axis=0)
    last = cum[:, length - 1:length]
    carried = carried_ref[...]
    up, down = jnp.exp(cum), jnp.exp(last - cum)
    d_up = dot(carried[:, :VAL_DIM], dm, ((1,), (0,))) * up
    d_down = dot(carried[:, VAL_DIM:], dm, ((1,), (0,))) * down
    dq_ref[...] = (join(dq) + d_up + d_down) * KEY_DIM ** (-0.5)
    dk_ref[...] = join(dk)
    dv_ref[...] = dot(dm, st_ref[...], ((1,), (1,)))
    dc_ref[...] = q * (join(dq_signed) + d_up - d_down) - k * join(dk_signed)
    dt_ref[...] = jnp.broadcast_to(
        jnp.sum(q * d_down, axis=1, keepdims=True), dt_ref.shape)


def last_kernel(me_ref, recv_ref, first_ref, carried_ref, k_ref, v_ref, cum_ref,
                pre_ref, speed_ref, dk_in_ref, dv_in_ref, dc_in_ref, dt_ref,
                dk_ref, dv_ref, logit_ref):
    length = k_ref.shape[1]
    me = me_ref[0]
    grad_bwd, grad_fwd = carry(
        recv_ref.shape[0], me, lambda i: recv_ref[i, :, :VAL_DIM].astype(F32),
        lambda i: jnp.exp(first_ref[i, :, 0:1]))
    k = k_ref[...].astype(F32)
    v = v_ref[...]
    cum = cum_ref[...]
    last = cum[:, length - 1:length]
    up, down = jnp.exp(cum), jnp.exp(last - cum)
    d_down = dot(grad_fwd, v, ((1,), (0,))) * down
    d_up = dot(grad_bwd, v, ((1,), (0,))) * up
    dk_ref[...] = dk_in_ref[...] + d_down + d_up
    dv_ref[...] = (dv_in_ref[...] + dot(grad_fwd, k * down, ((0,), (0,)))
                   + dot(grad_bwd, k * up, ((0,), (0,))))
    carried = carried_ref[...]
    grad_factor = jnp.sum(grad_fwd * carried[:, :VAL_DIM] + grad_bwd * carried[:, VAL_DIM:],
                          axis=1, keepdims=True)
    grad_total = (dt_ref[:, 0:1] + jnp.sum(k * d_down, axis=1, keepdims=True)
                  + grad_factor * jnp.exp(last))
    dc = dc_in_ref[...] + k * (d_up - d_down)
    from_here = triangle(length, lambda a, b: a >= b).astype(F32)
    grad_decay = exact_dot(dc, from_here) + grad_total
    pre = pre_ref[...].astype(F32)
    logit_ref[...] = grad_decay * speed_ref[...] * jax.nn.sigmoid(-pre)


def per_head(kernel, heads, outs, args, vmem_ops, scalars=0):
    def spec(shape):
        if len(shape) == 3:
            return pl.BlockSpec((shape[0], shape[1] // heads, shape[2]), lambda h: (0, h, 0))
        return pl.BlockSpec((shape[0] // heads, shape[1]), lambda h: (h, 0))

    in_specs = [pl.BlockSpec(memory_space=pltpu.SMEM)] * scalars
    in_specs += [spec(arg.shape) for arg in args[scalars:]]
    return pl.pallas_call(
        kernel,
        grid=(heads,),
        in_specs=in_specs,
        out_specs=[spec(shape) for shape, _ in outs],
        out_shape=[jax.ShapeDtypeStruct(shape, dtype) for shape, dtype in outs],
        cost_estimate=pl.CostEstimate(
            flops=vmem_ops * heads, bytes_accessed=1 << 20, transcendentals=0),
        compiler_params=pltpu.CompilerParams(dimension_semantics=("arbitrary",)),
    )(*args)


def body(
    queries,
    input_key_matrix,
    input_value_matrix,
    decay_preactivation,
    extra_log_decay,
    channel_decay_speed,
    output_weight_matrix,
    stored_expert_rows,
    chosen_expert_index,
    expert_combine_weight,
    cotangent,
    expert_gate_weight,
    expert_up_weight,
    expert_down_weight,
):
    heads = input_value_matrix.shape[0] // VAL_DIM
    tok_rows = queries.shape[1]
    experts, m = lax.axis_size("sp"), lax.axis_size("tp")
    index = lax.axis_index("sp")
    me = index.astype(jnp.int32).reshape(1)
    capacity = -(-(3 * tok_rows // experts) // 16) * 16
    slots = experts * capacity
    part_width = stored_expert_rows.shape[1]
    model_width = expert_gate_weight.shape[1]
    channels = heads * KEY_DIM
    values = heads * VAL_DIM
    tn = (((0,), (0,)), ((), ()))
    nt = (((1,), (1,)), ((), ()))
    gate_local, up_local, down_local = expert_gate_weight[0], expert_up_weight[0], expert_down_weight[0]
    (rows, hidden, grad_gate_pre, grad_up_pre, place, scores, cum, normed, inv_rms, mix_rows,
     carried, lasts) = dispatch(
        experts, m, capacity, queries, input_key_matrix, input_value_matrix,
        decay_preactivation, extra_log_decay, channel_decay_speed[None, :], stored_expert_rows,
        cotangent, chosen_expert_index.T, expert_combine_weight.T, gate_local, up_local, down_local)
    rows_x = rows[0].swapaxes(0, 1).reshape(slots, m * part_width)
    rows_dy = rows[1].swapaxes(0, 1).reshape(slots, m * part_width)
    carried = jnp.concatenate([carried[0].T, carried[1].T], axis=1)
    sums = lasts.swapaxes(1, 2)
    place = place.T
    speed = channel_decay_speed[:, None]
    state = ((channels, 2 * VAL_DIM), BF16)
    peer = lax.broadcasted_iota(jnp.int32, (experts, 1, 1), 0)
    all_mix = lax.all_to_all(jnp.broadcast_to(mix_rows[None], (experts, values, tok_rows)),
                             "sp", split_axis=0, concat_axis=0, tiled=True)
    partial_value = lax.dot_general(grad_gate_pre, gate_local, nt, preferred_element_type=F32)
    partial_value = partial_value + lax.dot_general(
        grad_up_pre, up_local, nt, preferred_element_type=F32
    )
    summed = lax.psum_scatter(
        partial_value.astype(BF16), "tp", scatter_dimension=1, tiled=True
    ).reshape(experts, capacity, part_width)
    grad_down = lax.dot_general(hidden, rows_dy, tn, preferred_element_type=F32).astype(BF16)
    grad_gate = lax.dot_general(rows_x, grad_gate_pre, tn, preferred_element_type=F32).astype(BF16)
    grad_up = lax.dot_general(rows_x, grad_up_pre, tn, preferred_element_type=F32).astype(BF16)
    summed, all_mix = lax.optimization_barrier((summed, all_mix))
    returned = lax.all_to_all(summed, "sp", split_axis=0, concat_axis=0, tiled=True)
    picked = jnp.dot(place, returned.reshape(slots, part_width), preferred_element_type=F32)
    grad_rows = (cotangent.astype(F32) + picked).astype(BF16)
    full_rows = lax.all_gather(grad_rows, "tp", axis=1, tiled=True)
    grad_normed = lax.dot_general(
        output_weight_matrix, full_rows, (((0,), (1,)), ((), ())), preferred_element_type=F32
    )
    grad_mixed, fwd_source, bwd_source = per_head(
        source_kernel, heads, [((values, tok_rows), F32), state, state],
        [grad_normed, normed, inv_rms, queries, cum], 1 << 26)
    sources = lax.all_to_all(jnp.where(peer < index, fwd_source[None], bwd_source[None]),
                             "sp", split_axis=0, concat_axis=0, tiled=True)
    by_channel = ((channels, tok_rows), F32)
    grad_queries, dk, dv, dc, dt = per_head(
        inner_kernel, heads,
        [by_channel, by_channel, ((values, tok_rows), F32), by_channel, by_channel],
        [grad_mixed, queries, input_key_matrix, input_value_matrix, cum, scores, carried],
        1 << 29)
    full_rows, dk = lax.optimization_barrier((full_rows, dk))
    rows_block = model_width // experts
    all_rows = lax.all_to_all(full_rows.reshape(tok_rows, experts, rows_block).swapaxes(0, 1),
                              "sp", split_axis=0, concat_axis=0, tiled=True)
    grad_out_proj = lax.dot_general(
        all_rows.reshape(experts * tok_rows, rows_block),
        all_mix.swapaxes(1, 2).reshape(experts * tok_rows, values),
        tn, preferred_element_type=F32)
    grad_keys, grad_values, grad_logit = per_head(
        last_kernel, heads, [by_channel, ((values, tok_rows), F32), by_channel],
        [me, sources, sums, carried, input_key_matrix, input_value_matrix, cum,
         decay_preactivation, speed, dk, dv, dc, dt], 1 << 26, scalars=1)
    return (
        grad_queries,
        grad_keys,
        grad_values,
        grad_logit,
        grad_out_proj,
        grad_gate[None],
        grad_up[None],
        grad_down[None],
    )


def solution(mesh):
    in_specs = (
        P("tp", "sp"),
        P("tp", "sp"),
        P("tp", "sp"),
        P("tp", "sp"),
        P("tp", "sp"),
        P("tp"),
        P(None, "tp"),
        P("sp", "tp"),
        P("sp", None),
        P("sp", None),
        P("sp", "tp"),
        P("sp", None, "tp"),
        P("sp", None, "tp"),
        P("sp", "tp", None),
    )
    out_specs = (
        P("tp", "sp"),
        P("tp", "sp"),
        P("tp", "sp"),
        P("tp", "sp"),
        P("sp", "tp"),
        P("sp", None, "tp"),
        P("sp", None, "tp"),
        P("sp", "tp", None),
    )
    return jax.shard_map(body, mesh=mesh, in_specs=in_specs, out_specs=out_specs, check_vma=False)
```

```python
import functools

import jax
import jax.numpy as jnp
from jax import lax
from jax.experimental import pallas as pl
from jax.experimental.pallas import tpu as pltpu
from jax.sharding import PartitionSpec as P

KEY_DIM = 32
VAL_DIM = 64
CORES = 2
BF16 = jnp.bfloat16
F32 = jnp.float32
MESH = pl.DeviceIdType.MESH
VMEM_LIMIT = 60 * 1024 * 1024
TN = ((0,), (0,))
NN = ((1,), (0,))
NT = ((1,), (1,))


def dot(a, b, contract):
    return lax.dot_general(a.astype(BF16), b.astype(BF16), (contract, ((), ())),
                           preferred_element_type=F32)


def exact_dot(a, b):
    return lax.dot_general(a, b, (((1,), (0,)), ((), ())), precision=lax.Precision.HIGHEST,
                           preferred_element_type=F32)


def triangle(length, test):
    rows = lax.broadcasted_iota(jnp.int32, (length, length), 0)
    cols = lax.broadcasted_iota(jnp.int32, (length, length), 1)
    return test(rows, cols)


def loop(count, step):
    lax.fori_loop(0, count, lambda i, _: (step(i), 0)[1], 0)


class Peers:
    def __init__(self, n, m):
        self.n, self.m, self.chips = n, m, m // CORES
        self.me, self.tp = lax.axis_index("sp"), lax.axis_index("tp")
        self.chip, self.core = lax.div(self.tp, CORES), lax.rem(self.tp, CORES)
        self.mate = self.chip * CORES + (1 - self.core)

    def to(self, d):
        return lax.rem(self.me + d, self.n)

    def source(self, d):
        return lax.rem(self.me - d + self.n, self.n)

    def to_chip(self, d):
        return lax.rem(self.chip + d, self.chips) * CORES + self.core

    def from_chip(self, d):
        return lax.rem(self.chip - d + self.chips, self.chips) * CORES + self.core

    def mate_from_chip(self, d):
        return lax.rem(self.chip - d + self.chips, self.chips) * CORES + (1 - self.core)

    def greet(self):
        barrier = pltpu.get_barrier_semaphore()

        def signal(device):
            pl.semaphore_signal(barrier, inc=1, device_id=device, device_id_type=MESH)

        loop(self.n - 1, lambda i: signal({"sp": self.to(i + 1)}))
        for d in range(1, self.chips):
            signal({"tp": self.to_chip(d)})
        signal({"tp": self.mate})

    def met(self):
        pl.semaphore_wait(pltpu.get_barrier_semaphore(), self.n - 1 + self.chips)


def copy_to(src, dst, send, recv, device):
    return pltpu.make_async_remote_copy(src_ref=src, dst_ref=dst, send_sem=send, recv_sem=recv,
                                        device_id=device, device_id_type=MESH)


def own_heads(stacked, width):
    heads = stacked.shape[0] // width
    head = lax.broadcasted_iota(jnp.int32, (width, stacked.shape[1]), 1) // KEY_DIM
    out = jnp.zeros((width, stacked.shape[1]), F32)
    for h in range(heads):
        out = jnp.where(head == h, stacked[h * width:(h + 1) * width], out)
    return out


def spread_heads(state, heads):
    head = lax.broadcasted_iota(jnp.int32, state.shape, 1) // KEY_DIM
    return jnp.concatenate([jnp.where(head == h, state, 0.0) for h in range(heads)], axis=0)


def as_row(column):
    length = column.shape[0]
    diagonal = triangle(length, lambda a, b: a == b)
    return jnp.sum(jnp.where(diagonal, column, 0.0), axis=0, keepdims=True)


def as_column(row):
    length = row.shape[1]
    diagonal = triangle(length, lambda a, b: a == b)
    return jnp.sum(jnp.where(diagonal, row, 0.0), axis=1, keepdims=True)


def carry(n, me, state_of, factor_of):
    shape = state_of(0).shape
    before, after = jnp.zeros(shape, F32), jnp.zeros(shape, F32)
    for i in range(n):
        before = jnp.where(i < me, before * factor_of(i) + state_of(i), before)
    for i in reversed(range(n)):
        after = jnp.where(i > me, after * factor_of(i) + state_of(i), after)
    return before, after


def dispatch_kernel(n, m, cap, q_ref, k_ref, v_ref, pre_ref, extra_ref, speed_ref, x_ref, cot_ref,
                    pick_ref, comb_ref, gate_any, up_any, down_any,
                    rows_ref, hidden_ref, ggp_ref, gup_ref, place_ref, st_ref, cum_ref,
                    normed_ref, inv_ref, mix_ref, carried_ref, last_ref,
                    send_ref, sbuf, sin, lbuf, inner_ref, gate_v, up_v, down_v, gp_ref, up_ref,
                    zs, zr, ys, yr, ps, pr, ss, sr, ws):
    at = Peers(n, m)
    me = at.me
    tok, channels = q_ref.shape[1], q_ref.shape[0]
    width = x_ref.shape[1]
    heads = channels // KEY_DIM
    slots = n * cap
    at.greet()
    loads = [pltpu.make_async_copy(src, dst, ws.at[i])
             for i, (src, dst) in enumerate(((gate_any, gate_v), (up_any, up_v),
                                             (down_any, down_v)))]
    for load in loads:
        load.start()

    expert = lax.broadcasted_iota(jnp.int32, (n, tok), 0)
    picks = [pick_ref[i:i + 1, :] == expert for i in range(2)]
    named = (picks[0] | picks[1]).astype(F32)
    counts = dot(named, triangle(tok, lambda a, b: a < b).astype(F32), NN)
    slot = lax.broadcasted_iota(jnp.int32, (slots, tok), 0)
    places = []
    for i in range(2):
        rank = jnp.sum(jnp.where(picks[i], counts, 0.0), axis=0, keepdims=True)
        places.append(slot == pick_ref[i:i + 1, :] * cap + rank.astype(jnp.int32))
    place = (places[0] | places[1]).astype(BF16)
    place_ref[...] = place
    weight = jnp.sum(jnp.where(places[0], comb_ref[0:1, :], 0.0)
                     + jnp.where(places[1], comb_ref[1:2, :], 0.0), axis=1, keepdims=True)
    send_ref[0] = dot(place, x_ref[...], NN).astype(BF16)
    send_ref[1] = (weight * dot(place, cot_ref[...], NN)).astype(BF16)

    def rows(p):
        return pl.ds(pl.multiple_of(p * cap, 16), cap)

    for t in range(2):
        rows_ref[t, at.tp, rows(me), :] = send_ref[t, rows(me), :]

    def out_row(t, d):
        p = at.to(d)
        return copy_to(send_ref.at[t, rows(p)], rows_ref.at[t, at.tp, rows(me)],
                       zs.at[t, d], zr.at[t, d], {"sp": p})

    def in_row(t, d):
        p = at.source(d)
        here = rows_ref.at[t, at.tp, rows(p)]
        return copy_to(here, here, zs.at[t, d], zr.at[t, d], {"sp": p})

    def across(t, d, dy):
        here = rows_ref.at[t, at.tp, rows(at.source(d))]
        return copy_to(here, here, ys.at[t, dy, d], yr.at[t, dy, d], {"tp": at.to_chip(dy)})

    def across_in(t, d, dy):
        here = rows_ref.at[t, at.from_chip(dy), rows(at.source(d))]
        return copy_to(here, here, ys.at[t, dy, d], yr.at[t, dy, d], {"tp": at.from_chip(dy)})

    def relay(t, d, dy):
        here = rows_ref.at[t, at.from_chip(dy), rows(at.source(d))]
        return copy_to(here, here, ps.at[t, dy, d], pr.at[t, dy, d], {"tp": at.mate})

    def relay_in(t, d, dy):
        here = rows_ref.at[t, at.mate_from_chip(dy), rows(at.source(d))]
        return copy_to(here, here, ps.at[t, dy, d], pr.at[t, dy, d], {"tp": at.mate})

    def pass_on(t, d):
        @pl.when(d > 0)
        def _():
            in_row(t, d).wait_recv()
        for dy in range(1, at.chips):
            across(t, d, dy).start()
        relay(t, d, 0).start()

    def pass_mate(t, d):
        for dy in range(1, at.chips):
            across_in(t, d, dy).wait_recv()
            relay(t, d, dy).start()

    def gathered(t, d):
        for dy in range(at.chips):
            relay_in(t, d, dy).wait_recv()

    at.met()
    for t in range(2):
        loop(n - 1, lambda i, t=t: out_row(t, i + 1).start())

    pre = pre_ref[...].astype(F32)
    log_sig = jnp.minimum(pre, 0.0) - jnp.log1p(jnp.exp(-jnp.abs(pre)))
    decays = as_column(speed_ref[...]) * log_sig + extra_ref[...]
    cum_ref[...] = exact_dot(decays, triangle(tok, lambda a, b: a <= b).astype(F32))

    per_head = -(-n // heads)

    def head(h):
        keys = pl.ds(pl.multiple_of(h * KEY_DIM, KEY_DIM), KEY_DIM)
        values = pl.ds(pl.multiple_of(h * VAL_DIM, VAL_DIM), VAL_DIM)
        q = q_ref[keys, :].astype(F32) * KEY_DIM ** (-0.5)
        cum = cum_ref[keys, :]
        cum_t = cum.T
        k_t = k_ref[keys, :].astype(F32).T
        total = jnp.zeros((tok, tok), F32)
        for c in range(KEY_DIM):
            decay = jnp.exp(-jnp.abs(cum_t[:, c:c + 1] - cum[c:c + 1, :]))
            total = total + (k_t[:, c:c + 1] * q[c:c + 1, :]) * decay
        scores = total.astype(BF16)
        st_ref[pl.ds(pl.multiple_of(h * tok, tok), tok), :] = scores
        inner_ref[values, :] = dot(v_ref[values, :], scores, NN)

        def forward(i):
            @pl.when(h * per_head + i < n)
            def _():
                pass_on(0, h * per_head + i)
        loop(per_head, forward)

    loop(heads, head)

    cum = cum_ref[...]
    last = cum[:, tok - 1:tok]
    k = k_ref[...].astype(F32)
    sbuf[0] = own_heads(dot(v_ref[...], k * jnp.exp(last - cum), NT), VAL_DIM).astype(BF16)
    sbuf[1] = own_heads(dot(v_ref[...], k * jnp.exp(cum), NT), VAL_DIM).astype(BF16)
    lbuf[...] = jnp.broadcast_to(as_row(last), lbuf.shape)
    sin[me] = jnp.zeros(sin.shape[1:], BF16)
    last_ref[me] = jnp.zeros(last_ref.shape[1:], F32)

    def out_state(d):
        p = at.to(d)
        return (copy_to(sbuf.at[jnp.where(p > me, 0, 1)], sin.at[me], ss.at[0, d], sr.at[0, d],
                        {"sp": p}),
                copy_to(lbuf, last_ref.at[me], ss.at[1, d], sr.at[1, d], {"sp": p}))

    def in_state(d):
        p = at.source(d)
        return (copy_to(sbuf.at[0], sin.at[p], ss.at[0, d], sr.at[0, d], {"sp": p}),
                copy_to(lbuf, last_ref.at[p], ss.at[1, d], sr.at[1, d], {"sp": p}))

    loop(n - 1, lambda i: [copy.start() for copy in out_state(i + 1)] and None)

    half = n // 2
    loop(n, lambda d: pass_mate(0, d))
    loop(half, lambda d: pass_on(1, d))
    loop(n, lambda d: gathered(0, d))

    def columns_of(weights, t):
        total = None
        for j in range(m):
            part = dot(rows_ref[t, j], weights[j * width:(j + 1) * width, :], NN)
            total = part if total is None else total + part
        return total

    loads[0].wait()
    gp_ref[...] = columns_of(gate_v, 0)
    loop(n - half, lambda d: pass_on(1, d + half))
    loads[1].wait()
    up_ref[...] = columns_of(up_v, 0)
    loop(n, lambda d: pass_mate(1, d))

    loop(n - 1, lambda i: [copy.wait_recv() for copy in in_state(i + 1)] and None)
    before, after = carry(n, me, lambda i: sin[i].astype(F32),
                          lambda i: jnp.exp(last_ref[i, 0:1, :]))
    carried_ref[0] = before
    carried_ref[1] = after
    q = q_ref[...].astype(F32) * KEY_DIM ** (-0.5)
    mixed = inner_ref[...] + dot(spread_heads(before, heads), q * jnp.exp(cum), NN)
    mixed = mixed + dot(spread_heads(after, heads), q * jnp.exp(last - cum), NN)
    for h in range(heads):
        part = mixed[h * VAL_DIM:(h + 1) * VAL_DIM]
        inv = lax.rsqrt(jnp.mean(part * part, axis=0, keepdims=True) + 1e-06)
        normed = part * inv
        normed_ref[h * VAL_DIM:(h + 1) * VAL_DIM, :] = normed
        mix_ref[h * VAL_DIM:(h + 1) * VAL_DIM, :] = normed.astype(BF16)
        inv_ref[h * 8:(h + 1) * 8, :] = jnp.broadcast_to(inv, (8, tok))

    loop(n, lambda d: gathered(1, d))
    loads[2].wait()
    grad_hidden = None
    for j in range(m):
        part = dot(rows_ref[1, j], down_v[:, j * width:(j + 1) * width], NT)
        grad_hidden = part if grad_hidden is None else grad_hidden + part
    gate_pre, up_pre = gp_ref[...], up_ref[...]
    gate_sig = jax.nn.sigmoid(gate_pre)
    gate_act = gate_pre * gate_sig
    hidden_ref[...] = (gate_act * up_pre).astype(BF16)
    ggp_ref[...] = (grad_hidden * up_pre * gate_sig
                    * (1.0 + gate_pre * (1.0 - gate_sig))).astype(BF16)
    gup_ref[...] = (grad_hidden * gate_act).astype(BF16)

    def drain(i):
        for copy in out_state(i + 1):
            copy.wait_send()
        for t in range(2):
            out_row(t, i + 1).wait_send()
    loop(n - 1, drain)

    def drain_passed(d):
        for t in range(2):
            for dy in range(1, at.chips):
                across(t, d, dy).wait_send()
            for dy in range(at.chips):
                relay(t, d, dy).wait_send()
    loop(n, drain_passed)


def vmem_specs(count):
    return [pl.BlockSpec(memory_space=pltpu.VMEM)] * count


def dispatch(n, m, cap, q, k, v, pre, extra, speed, x, cot, picks, comb, gate, up, down):
    channels, tok = q.shape
    values = v.shape[0]
    heads = channels // KEY_DIM
    slots, width, units = n * cap, x.shape[1], gate.shape[1]
    chips = m // CORES
    dma = pltpu.SemaphoreType.DMA
    outs = [((2, m, slots, width), BF16), ((slots, units), BF16), ((slots, units), BF16),
            ((slots, units), BF16), ((slots, tok), BF16), ((heads * tok, tok), BF16),
            ((channels, tok), F32), ((values, tok), F32), ((heads * 8, tok), F32),
            ((values, tok), BF16), ((2, VAL_DIM, channels), F32), ((n, 8, channels), F32)]
    return pl.pallas_call(
        functools.partial(dispatch_kernel, n, m, cap),
        in_specs=vmem_specs(10) + [pl.BlockSpec(memory_space=pl.ANY)] * 3,
        out_specs=vmem_specs(len(outs)),
        out_shape=[jax.ShapeDtypeStruct(shape, dtype) for shape, dtype in outs],
        scratch_shapes=[
            pltpu.VMEM((2, slots, width), BF16), pltpu.VMEM((2, VAL_DIM, channels), BF16),
            pltpu.VMEM((n, VAL_DIM, channels), BF16), pltpu.VMEM((8, channels), F32),
            pltpu.VMEM((values, tok), F32),
            pltpu.VMEM(gate.shape, BF16), pltpu.VMEM(up.shape, BF16), pltpu.VMEM(down.shape, BF16),
            pltpu.VMEM((slots, units), F32), pltpu.VMEM((slots, units), F32),
            dma((2, n)), dma((2, n)), dma((2, chips, n)), dma((2, chips, n)),
            dma((2, chips, n)), dma((2, chips, n)), dma((2, n)), dma((2, n)), dma((3,)),
        ],
        compiler_params=pltpu.CompilerParams(collective_id=0, has_side_effects=True,
                                             vmem_limit_bytes=VMEM_LIMIT),
        name="dispatch",
    )(q, k, v, pre, extra, speed, x, cot, picks, comb, gate, up, down)


def combine_kernel(n, m, cap, rows_ref, hidden_ref, ggp_ref, gup_ref, place_ref, cot_ref, mix_ref,
                   gate_any, up_any,
                   full_ref, dgate_ref, dup_ref, ddown_ref, all_mix_ref,
                   gate_v, up_v, own_ref, psend, pin, ybuf, yin, zbuf, ret_ref,
                   ps, pr, ys, yr, zs, zr, fs, fr, ms, mr, ws):
    at = Peers(n, m)
    me = at.me
    width = cot_ref.shape[1]
    at.greet()
    loads = [pltpu.make_async_copy(src, dst, ws.at[i])
             for i, (src, dst) in enumerate(((gate_any, gate_v), (up_any, up_v)))]
    for load in loads:
        load.start()

    def rows(p):
        return pl.ds(pl.multiple_of(p * cap, 16), cap)

    def partial(j):
        block = pl.ds(pl.multiple_of(j * width, width), width)
        return dot(ggp_ref[...], gate_v[block, :], NT) + dot(gup_ref[...], up_v[block, :], NT)

    def pair(dy):
        return copy_to(psend.at[dy], pin.at[dy], ps.at[dy], pr.at[dy], {"tp": at.mate})

    def column_of(dy, core):
        return lax.rem(at.chip + dy, at.chips) * CORES + core

    def across(d, dy):
        r = rows(at.to(d))
        return copy_to(ybuf.at[dy, r], yin.at[dy, r], ys.at[dy, d], yr.at[dy, d],
                       {"tp": at.to_chip(dy)})

    def across_in(d, dy):
        r = rows(at.to(d))
        return copy_to(yin.at[dy, r], yin.at[dy, r], ys.at[dy, d], yr.at[dy, d],
                       {"tp": at.from_chip(dy)})

    def back(d):
        return copy_to(zbuf.at[rows(at.to(d))], ret_ref.at[rows(me)], zs.at[d], zr.at[d],
                       {"sp": at.to(d)})

    def back_in(d):
        here = ret_ref.at[rows(at.source(d))]
        return copy_to(here, here, zs.at[d], zr.at[d], {"sp": at.source(d)})

    def mix_out(d):
        return copy_to(mix_ref, all_mix_ref.at[me], ms.at[d], mr.at[d], {"sp": at.to(d)})

    def mix_in(d):
        p = at.source(d)
        return copy_to(mix_ref, all_mix_ref.at[p], ms.at[d], mr.at[d], {"sp": p})

    all_mix_ref[me] = mix_ref[...]
    loads[0].wait()
    loads[1].wait()
    order = list(range(1, at.chips)) + [0]
    for i, dy in enumerate(order):
        psend[dy] = partial(column_of(dy, 1 - at.core)).astype(BF16)
        if i == 0:
            at.met()
        pair(dy).start()
        if i == 0:
            loop(n - 1, lambda i: mix_out(i + 1).start())
        own_ref[dy] = partial(column_of(dy, at.core))
        if dy > 0:
            pair(dy).wait_recv()
            ybuf[dy] = (own_ref[dy] + pin[dy].astype(F32)).astype(BF16)
            loop(n, lambda d, dy=dy: across(lax.rem(d + 1, n), dy).start())
    pair(0).wait_recv()
    own_ref[0] = own_ref[0] + pin[0].astype(F32)

    pieces = []
    for j in range(m):
        cols = slice(j * width, (j + 1) * width)

        def gate_piece(j=j, cols=cols):
            dgate_ref[cols, :] = dot(rows_ref[0, j], ggp_ref[...], TN).astype(BF16)

        def up_piece(j=j, cols=cols):
            dup_ref[cols, :] = dot(rows_ref[0, j], gup_ref[...], TN).astype(BF16)

        def down_piece(j=j, cols=cols):
            ddown_ref[:, cols] = dot(hidden_ref[...], rows_ref[1, j], TN).astype(BF16)
        pieces += [gate_piece, up_piece, down_piece]

    steps = n + 4
    done = 0
    for i in range(n):
        upto = len(pieces) * (i + 1) // steps
        for piece in pieces[done:upto]:
            piece()
        done = upto
        d = (i + 1) % n
        r = rows(at.to(d))
        total = own_ref[0, r, :]
        for dy in range(1, at.chips):
            across_in(d, dy).wait_recv()
            total = total + yin[dy, r, :].astype(F32)
        if d == 0:
            ret_ref[r, :] = total.astype(BF16)
        else:
            zbuf[r, :] = total.astype(BF16)
            back(d).start()
    upto = len(pieces) * (n + 2) // steps
    for piece in pieces[done:upto]:
        piece()
    loop(n - 1, lambda i: back_in(i + 1).wait_recv())
    picked = dot(place_ref[...], ret_ref[...], TN)
    full_ref[at.tp] = (cot_ref[...].astype(F32) + picked).astype(BF16)

    def share(dy):
        here = full_ref.at[at.tp]
        return copy_to(here, here, fs.at[0, dy], fr.at[0, dy],
                       {"tp": at.to_chip(dy)} if dy else {"tp": at.mate})

    def share_in(dy):
        here = full_ref.at[at.from_chip(dy) if dy else at.mate]
        return copy_to(here, here, fs.at[0, dy], fr.at[0, dy], {"tp": at.mate})

    def relay(dy):
        here = full_ref.at[at.from_chip(dy)]
        return copy_to(here, here, fs.at[1, dy], fr.at[1, dy], {"tp": at.mate})

    def relay_in(dy):
        here = full_ref.at[at.mate_from_chip(dy)]
        return copy_to(here, here, fs.at[1, dy], fr.at[1, dy], {"tp": at.mate})

    for dy in order:
        share(dy).start()
    for piece in pieces[upto:]:
        piece()
    for dy in range(1, at.chips):
        share_in(dy).wait_recv()
        relay(dy).start()
    share_in(0).wait_recv()
    for dy in range(1, at.chips):
        relay_in(dy).wait_recv()
    for dy in range(at.chips):
        pair(dy).wait_send()
        share(dy).wait_send()
    for dy in range(1, at.chips):
        relay(dy).wait_send()
        loop(n, lambda d, dy=dy: across(d, dy).wait_send())
    loop(n - 1, lambda i: back(i + 1).wait_send())
    loop(n - 1, lambda i: mix_out(i + 1).wait_send())
    loop(n - 1, lambda i: mix_in(i + 1).wait_recv())


def combine(n, m, cap, rows, hidden, ggp, gup, place, cot, mix, gate, up):
    slots, units = hidden.shape
    tok, width = cot.shape
    chips = m // CORES
    dma = pltpu.SemaphoreType.DMA
    outs = [((m, tok, width), BF16), (gate.shape, BF16), (up.shape, BF16),
            ((units, m * width), BF16), ((n,) + mix.shape, BF16)]
    return pl.pallas_call(
        functools.partial(combine_kernel, n, m, cap),
        in_specs=vmem_specs(7) + [pl.BlockSpec(memory_space=pl.ANY)] * 2,
        out_specs=vmem_specs(len(outs)),
        out_shape=[jax.ShapeDtypeStruct(shape, dtype) for shape, dtype in outs],
        scratch_shapes=[
            pltpu.VMEM(gate.shape, BF16), pltpu.VMEM(up.shape, BF16),
            pltpu.VMEM((chips, slots, width), F32), pltpu.VMEM((chips, slots, width), BF16),
            pltpu.VMEM((chips, slots, width), BF16), pltpu.VMEM((chips, slots, width), BF16),
            pltpu.VMEM((chips, slots, width), BF16), pltpu.VMEM((slots, width), BF16),
            pltpu.VMEM((slots, width), BF16),
            dma((chips,)), dma((chips,)), dma((chips, n)), dma((chips, n)), dma((n,)), dma((n,)),
            dma((2, chips)), dma((2, chips)), dma((n,)), dma((n,)), dma((2,)),
        ],
        compiler_params=pltpu.CompilerParams(collective_id=1, has_side_effects=True,
                                             vmem_limit_bytes=VMEM_LIMIT),
        name="combine",
    )(rows, hidden, ggp, gup, place, cot, mix, gate, up)


def finish_kernel(n, m, project, *refs):
    (full_ref, wo_ref, normed_ref, inv_ref, q_ref, k_ref, v_ref, pre_ref, speed_ref, cum_ref,
     st_ref, carried_ref, last_ref) = refs[:13]
    refs = refs[13:]
    if project:
        mix_ref, refs = refs[0], refs[1:]
    dq_ref, dk_ref, dv_ref, logit_ref = refs[:4]
    refs = refs[4:]
    if project:
        proj_ref, refs = refs[0], refs[1:]
    dm_ref, dc_ref, sbuf, sin, ss, sr = refs[:6]
    if project:
        psend, prow, zs, zr, fs, fr = refs[6:]
    at = Peers(n, m)
    me = at.me
    channels, tok = q_ref.shape
    values = v_ref.shape[0]
    heads = channels // KEY_DIM
    width = full_ref.shape[2]
    at.greet()

    def exchange(d):
        p = at.to(d)
        return copy_to(sbuf.at[jnp.where(p < me, 0, 1)], sin.at[me], ss.at[d], sr.at[d],
                       {"sp": p})

    def exchange_in(d):
        p = at.source(d)
        return copy_to(sbuf.at[0], sin.at[p], ss.at[d], sr.at[d], {"sp": p})

    gn = None
    for j in range(m):
        part = dot(full_ref[j], wo_ref[j * width:(j + 1) * width, :], NN)
        gn = part if gn is None else gn + part
    gn = gn.T
    for h in range(heads):
        block = slice(h * VAL_DIM, (h + 1) * VAL_DIM)
        normed, g = normed_ref[block, :], gn[block]
        dm_ref[block, :] = inv_ref[h * 8:h * 8 + 1, :] * (
            g - normed * jnp.mean(g * normed, axis=0, keepdims=True))
    cum = cum_ref[...]
    last = cum[:, tok - 1:tok]
    up, down = jnp.exp(cum), jnp.exp(last - cum)
    scale = KEY_DIM ** (-0.5)
    q = q_ref[...].astype(F32) * scale
    dm = dm_ref[...]
    sbuf[0] = own_heads(dot(dm, q * up, NT), VAL_DIM).astype(BF16)
    sbuf[1] = own_heads(dot(dm, q * down, NT), VAL_DIM).astype(BF16)
    sin[me] = jnp.zeros(sin.shape[1:], BF16)
    if project:
        block = proj_ref.shape[0]
        share = tok // m
        row = lax.broadcasted_iota(jnp.int32, (share, tok), 0) + at.tp * share
        chosen = (row == lax.broadcasted_iota(jnp.int32, (share, tok), 1)).astype(BF16)
        per = width // block
        for j in range(m):
            part = dot(chosen, full_ref[j], NN).astype(BF16)
            for i in range(per):
                psend[j * per + i] = part[:, i * block:(i + 1) * block]

        def share_of(j):
            return pl.ds(pl.multiple_of(j * share, 16), share)

        def rows_out(d):
            p = at.to(d)
            return copy_to(psend.at[p], prow.at[me, share_of(at.tp)], zs.at[d], zr.at[d],
                           {"sp": p})

        def rows_in(d):
            here = prow.at[at.source(d), share_of(at.tp)]
            return copy_to(here, here, zs.at[d], zr.at[d], {"sp": at.source(d)})

        def spread(dy):
            here = prow.at[:, share_of(at.tp)]
            return copy_to(here, here, fs.at[0, dy], fr.at[0, dy],
                           {"tp": at.to_chip(dy)} if dy else {"tp": at.mate})

        def spread_in(dy):
            here = prow.at[:, share_of(at.from_chip(dy) if dy else at.mate)]
            return copy_to(here, here, fs.at[0, dy], fr.at[0, dy], {"tp": at.mate})

        def relay(dy):
            here = prow.at[:, share_of(at.from_chip(dy))]
            return copy_to(here, here, fs.at[1, dy], fr.at[1, dy], {"tp": at.mate})

        def relay_in(dy):
            here = prow.at[:, share_of(at.mate_from_chip(dy))]
            return copy_to(here, here, fs.at[1, dy], fr.at[1, dy], {"tp": at.mate})

        prow[me, share_of(at.tp), :] = psend[me]
    at.met()
    loop(n - 1, lambda i: exchange(i + 1).start())
    if project:
        loop(n - 1, lambda i: rows_out(i + 1).start())

    row = lax.broadcasted_iota(jnp.int32, (tok, tok), 0)
    col = lax.broadcasted_iota(jnp.int32, (tok, tok), 1)
    sign = jnp.where(row > col, 1.0, jnp.where(row < col, -1.0, 0.0)).astype(F32)

    def head(h):
        keys = pl.ds(pl.multiple_of(h * KEY_DIM, KEY_DIM), KEY_DIM)
        vals = pl.ds(pl.multiple_of(h * VAL_DIM, VAL_DIM), VAL_DIM)
        dm, v, cum = dm_ref[vals, :], v_ref[vals, :], cum_ref[keys, :]
        q = q_ref[keys, :].astype(F32) * scale
        k = k_ref[keys, :].astype(F32)
        by_query = dot(dm, v, TN)
        by_key = dot(v, dm, TN)
        by_query_signed = by_query * sign
        by_key_signed = by_key * -sign
        cum_t, q_t, k_t = cum.T, q.T, k.T
        dq, dk, dq_signed, dk_signed = [], [], [], []
        for c in range(KEY_DIM):
            weight = jnp.exp(-jnp.abs(cum_t[:, c:c + 1] - cum[c:c + 1, :]))
            with_q = weight * q_t[:, c:c + 1]
            with_k = weight * k_t[:, c:c + 1]
            dk.append(jnp.sum(by_query * with_q, axis=0, keepdims=True))
            dk_signed.append(jnp.sum(by_query_signed * with_q, axis=0, keepdims=True))
            dq.append(jnp.sum(by_key * with_k, axis=0, keepdims=True))
            dq_signed.append(jnp.sum(by_key_signed * with_k, axis=0, keepdims=True))
        join = lambda parts: jnp.concatenate(parts, axis=0)
        dq_ref[keys, :] = join(dq)
        dk_ref[keys, :] = join(dk)
        dv_ref[vals, :] = dot(dm, st_ref[pl.ds(pl.multiple_of(h * tok, tok), tok), :], NT)
        dc_ref[keys, :] = q * join(dq_signed) - k * join(dk_signed)

    early = heads // 2
    loop(early, head)
    if project:
        loop(n - 1, lambda i: rows_in(i + 1).wait_recv())
        for dy in range(at.chips):
            spread(dy).start()
    loop(heads - early, lambda h: head(h + early))
    if project:
        for dy in range(1, at.chips):
            spread_in(dy).wait_recv()
            relay(dy).start()

    k = k_ref[...].astype(F32)
    in_fwd, in_bwd = carried_ref[0], carried_ref[1]
    d_up = dot(spread_heads(in_fwd, heads), dm, TN) * up
    d_down = dot(spread_heads(in_bwd, heads), dm, TN) * down
    dq_ref[...] = (dq_ref[...] + d_up + d_down) * scale
    dc = dc_ref[...] + q * (d_up - d_down)
    total = jnp.sum(q * d_down, axis=1, keepdims=True)

    loop(n - 1, lambda i: exchange_in(i + 1).wait_recv())
    grad_bwd, grad_fwd = carry(n, me, lambda i: sin[i].astype(F32),
                               lambda i: jnp.exp(last_ref[i, 0:1, :]))
    wide_fwd, wide_bwd = spread_heads(grad_fwd, heads), spread_heads(grad_bwd, heads)
    v = v_ref[...]
    d_down = dot(wide_fwd, v, TN) * down
    d_up = dot(wide_bwd, v, TN) * up
    dk_ref[...] = dk_ref[...] + d_down + d_up
    dv_ref[...] = dv_ref[...] + dot(wide_fwd, k * down, NN) + dot(wide_bwd, k * up, NN)
    factor = as_column(jnp.sum(grad_fwd * in_fwd + grad_bwd * in_bwd, axis=0, keepdims=True))
    total = total + jnp.sum(k * d_down, axis=1, keepdims=True) + factor * jnp.exp(last)
    dc = dc + k * (d_up - d_down)
    decay = exact_dot(dc, triangle(tok, lambda a, b: a >= b).astype(F32)) + total
    logit_ref[...] = decay * as_column(speed_ref[...]) * jax.nn.sigmoid(
        -pre_ref[...].astype(F32))

    if project:
        spread_in(0).wait_recv()
        for dy in range(1, at.chips):
            relay_in(dy).wait_recv()
        out = None
        for s in range(n):
            part = dot(mix_ref[s], prow[s], NN)
            out = part if out is None else out + part
        proj_ref[...] = out.T
        for dy in range(at.chips):
            spread(dy).wait_send()
        for dy in range(1, at.chips):
            relay(dy).wait_send()
        loop(n - 1, lambda i: rows_out(i + 1).wait_send())
    loop(n - 1, lambda i: exchange(i + 1).wait_send())


def finish(n, m, project, full, wo, normed, inv, q, k, v, pre, speed, cum, st, carried, lasts,
           all_mix):
    channels, tok = q.shape
    values = v.shape[0]
    block = wo.shape[0] // n
    chips = m // CORES
    dma = pltpu.SemaphoreType.DMA
    outs = [((channels, tok), F32), ((channels, tok), F32), ((values, tok), F32),
            ((channels, tok), F32)]
    scratch = [pltpu.VMEM((values, tok), F32), pltpu.VMEM((channels, tok), F32),
               pltpu.VMEM((2, VAL_DIM, channels), BF16), pltpu.VMEM((n, VAL_DIM, channels), BF16),
               dma((n,)), dma((n,))]
    args = [full, wo, normed, inv, q, k, v, pre, speed, cum, st, carried, lasts]
    if project:
        args.append(all_mix)
        outs.append(((block, values), F32))
        scratch += [pltpu.VMEM((n, tok // m, block), BF16), pltpu.VMEM((n, tok, block), BF16),
                    dma((n,)), dma((n,)), dma((2, chips)), dma((2, chips))]
    return pl.pallas_call(
        functools.partial(finish_kernel, n, m, project),
        in_specs=vmem_specs(len(args)),
        out_specs=vmem_specs(len(outs)),
        out_shape=[jax.ShapeDtypeStruct(shape, dtype) for shape, dtype in outs],
        scratch_shapes=scratch,
        compiler_params=pltpu.CompilerParams(collective_id=2, has_side_effects=True,
                                             vmem_limit_bytes=VMEM_LIMIT),
        name="finish",
    )(*args)


def body(
    queries,
    input_key_matrix,
    input_value_matrix,
    decay_preactivation,
    extra_log_decay,
    channel_decay_speed,
    output_weight_matrix,
    stored_expert_rows,
    chosen_expert_index,
    expert_combine_weight,
    cotangent,
    expert_gate_weight,
    expert_up_weight,
    expert_down_weight,
):
    heads = input_value_matrix.shape[0] // VAL_DIM
    tok_rows = queries.shape[1]
    experts, m = lax.axis_size("sp"), lax.axis_size("tp")
    capacity = -(-(3 * tok_rows // experts) // 16) * 16
    slots = experts * capacity
    part_width = stored_expert_rows.shape[1]
    gate_local, up_local, down_local = expert_gate_weight[0], expert_up_weight[0], expert_down_weight[0]
    (rows, hidden, grad_gate_pre, grad_up_pre, place, scores, cum, normed, inv_rms, mix_rows,
     carried, lasts) = dispatch(
        experts, m, capacity, queries, input_key_matrix, input_value_matrix,
        decay_preactivation, extra_log_decay, channel_decay_speed[None, :], stored_expert_rows,
        cotangent, chosen_expert_index.T, expert_combine_weight.T, gate_local, up_local, down_local)
    full, grad_gate, grad_up, grad_down, all_mix = combine(
        experts, m, capacity, rows, hidden, grad_gate_pre, grad_up_pre, place, cotangent,
        mix_rows, gate_local, up_local)
    rows_block = output_weight_matrix.shape[0] // experts
    project = (tok_rows % (16 * m) == 0 and rows_block % 128 == 0
               and part_width % rows_block == 0)
    grads = finish(
        experts, m, project, full, output_weight_matrix, normed, inv_rms, queries,
        input_key_matrix, input_value_matrix, decay_preactivation, channel_decay_speed[None, :],
        cum, scores, carried, lasts, all_mix)
    grad_queries, grad_keys, grad_values, grad_logit = grads[:4]
    if project:
        grad_out_proj = grads[4]
    else:
        full_rows = full.swapaxes(0, 1).reshape(tok_rows, experts, rows_block)
        all_rows = lax.all_to_all(full_rows.swapaxes(0, 1), "sp", split_axis=0, concat_axis=0,
                                  tiled=True)
        grad_out_proj = jnp.einsum("str,sct->rc", all_rows, all_mix, preferred_element_type=F32)
    return (
        grad_queries,
        grad_keys,
        grad_values,
        grad_logit,
        grad_out_proj,
        grad_gate[None],
        grad_up[None],
        grad_down[None],
    )


def solution(mesh):
    in_specs = (
        P("tp", "sp"),
        P("tp", "sp"),
        P("tp", "sp"),
        P("tp", "sp"),
        P("tp", "sp"),
        P("tp"),
        P(None, "tp"),
        P("sp", "tp"),
        P("sp", None),
        P("sp", None),
        P("sp", "tp"),
        P("sp", None, "tp"),
        P("sp", None, "tp"),
        P("sp", "tp", None),
    )
    out_specs = (
        P("tp", "sp"),
        P("tp", "sp"),
        P("tp", "sp"),
        P("tp", "sp"),
        P("sp", "tp"),
        P("sp", None, "tp"),
        P("sp", None, "tp"),
        P("sp", "tp", None),
    )
    return jax.shard_map(body, mesh=mesh, in_specs=in_specs, out_specs=out_specs, check_vma=False)
```

```python
import functools

import jax
import jax.numpy as jnp
from jax import lax
from jax.experimental import pallas as pl
from jax.experimental.pallas import tpu as pltpu
from jax.sharding import PartitionSpec as P

KEY_DIM = 32
VAL_DIM = 64
CORES = 2
BF16 = jnp.bfloat16
F32 = jnp.float32
MESH = pl.DeviceIdType.MESH
VMEM_LIMIT = 28 * 1024 * 1024
TN = ((0,), (0,))
NN = ((1,), (0,))
NT = ((1,), (1,))


def dot(a, b, contract):
    return lax.dot_general(a.astype(BF16), b.astype(BF16), (contract, ((), ())),
                           preferred_element_type=F32)


def exact_dot(a, b):
    return lax.dot_general(a, b, (((1,), (0,)), ((), ())), precision=lax.Precision.HIGHEST,
                           preferred_element_type=F32)


def triangle(length, test):
    rows = lax.broadcasted_iota(jnp.int32, (length, length), 0)
    cols = lax.broadcasted_iota(jnp.int32, (length, length), 1)
    return test(rows, cols)


def loop(count, step):
    lax.fori_loop(0, count, lambda i, _: (step(i), 0)[1], 0)


class Peers:
    def __init__(self, n, m):
        self.n, self.m, self.chips = n, m, m // CORES
        self.me, self.tp = lax.axis_index("sp"), lax.axis_index("tp")
        self.chip, self.core = lax.div(self.tp, CORES), lax.rem(self.tp, CORES)
        self.mate = self.chip * CORES + (1 - self.core)

    def to(self, d):
        return lax.rem(self.me + d, self.n)

    def source(self, d):
        return lax.rem(self.me - d + self.n, self.n)

    def to_chip(self, d):
        return lax.rem(self.chip + d, self.chips) * CORES + self.core

    def from_chip(self, d):
        return lax.rem(self.chip - d + self.chips, self.chips) * CORES + self.core

    def mate_from_chip(self, d):
        return lax.rem(self.chip - d + self.chips, self.chips) * CORES + (1 - self.core)

    def greet(self):
        barrier = pltpu.get_barrier_semaphore()

        def signal(device):
            pl.semaphore_signal(barrier, inc=1, device_id=device, device_id_type=MESH)

        loop(self.n - 1, lambda i: signal({"sp": self.to(i + 1)}))
        for d in range(1, self.chips):
            signal({"tp": self.to_chip(d)})
        signal({"tp": self.mate})

    def met(self):
        pl.semaphore_wait(pltpu.get_barrier_semaphore(), self.n - 1 + self.chips)


def copy_to(src, dst, send, recv, device):
    return pltpu.make_async_remote_copy(src_ref=src, dst_ref=dst, send_sem=send, recv_sem=recv,
                                        device_id=device, device_id_type=MESH)


def own_heads(stacked, width):
    heads = stacked.shape[0] // width
    head = lax.broadcasted_iota(jnp.int32, (width, stacked.shape[1]), 1) // KEY_DIM
    out = jnp.zeros((width, stacked.shape[1]), F32)
    for h in range(heads):
        out = jnp.where(head == h, stacked[h * width:(h + 1) * width], out)
    return out


def spread_heads(state, heads):
    head = lax.broadcasted_iota(jnp.int32, state.shape, 1) // KEY_DIM
    return jnp.concatenate([jnp.where(head == h, state, 0.0) for h in range(heads)], axis=0)


def as_row(column):
    length = column.shape[0]
    diagonal = triangle(length, lambda a, b: a == b)
    return jnp.sum(jnp.where(diagonal, column, 0.0), axis=0, keepdims=True)


def as_column(row):
    length = row.shape[1]
    diagonal = triangle(length, lambda a, b: a == b)
    return jnp.sum(jnp.where(diagonal, row, 0.0), axis=1, keepdims=True)


def carry(n, me, state_of, factor_of):
    shape = state_of(0).shape
    before, after = jnp.zeros(shape, F32), jnp.zeros(shape, F32)
    for i in range(n):
        before = jnp.where(i < me, before * factor_of(i) + state_of(i), before)
    for i in reversed(range(n)):
        after = jnp.where(i > me, after * factor_of(i) + state_of(i), after)
    return before, after


def dispatch_kernel(n, m, cap, q_any, k_any, v_any, pre_any, extra_any, speed_any, x_any, cot_any,
                    pick_any, comb_any, gate_any, up_any, down_any,
                    rows_ref, hidden_ref, ggp_ref, gup_ref, place_ref, st_ref, cum_ref,
                    normed_ref, inv_ref, mix_ref, carried_ref, last_ref, gate_v, up_v,
                    q_ref, k_ref, v_ref, pre_ref, speed_ref, cot_ref,
                    extra_ref, x_ref, pick_ref, comb_ref, send_ref, sbuf, sin, lbuf, inner_ref, down_v, gp_ref, up_ref,
                    zs, zr, ys, yr, ps, pr, ss, sr, ws):
    at = Peers(n, m)
    me = at.me
    tok, channels = q_ref.shape[1], q_ref.shape[0]
    width = x_ref.shape[1]
    heads = channels // KEY_DIM
    slots = n * cap
    held = ((pick_any, pick_ref), (comb_any, comb_ref), (x_any, x_ref), (cot_any, cot_ref),
            (pre_any, pre_ref), (extra_any, extra_ref), (speed_any, speed_ref), (q_any, q_ref),
            (k_any, k_ref), (v_any, v_ref), (gate_any, gate_v), (up_any, up_v),
            (down_any, down_v))
    loads = [pltpu.make_async_copy(src, dst, ws.at[i]) for i, (src, dst) in enumerate(held)]
    for load in loads:
        load.start()
    at.greet()
    for load in loads[:4]:
        load.wait()

    expert = lax.broadcasted_iota(jnp.int32, (n, tok), 0)
    picks = [pick_ref[i:i + 1, :] == expert for i in range(2)]
    named = (picks[0] | picks[1]).astype(F32)
    counts = dot(named, triangle(tok, lambda a, b: a < b).astype(F32), NN)
    slot = lax.broadcasted_iota(jnp.int32, (slots, tok), 0)
    places = []
    for i in range(2):
        rank = jnp.sum(jnp.where(picks[i], counts, 0.0), axis=0, keepdims=True)
        places.append(slot == pick_ref[i:i + 1, :] * cap + rank.astype(jnp.int32))
    place = (places[0] | places[1]).astype(BF16)
    place_ref[...] = place
    weight = jnp.sum(jnp.where(places[0], comb_ref[0:1, :], 0.0)
                     + jnp.where(places[1], comb_ref[1:2, :], 0.0), axis=1, keepdims=True)
    send_ref[0] = dot(place, x_ref[...], NN).astype(BF16)
    send_ref[1] = (weight * dot(place, cot_ref[...], NN)).astype(BF16)

    def rows(p):
        return pl.ds(pl.multiple_of(p * cap, 16), cap)

    for t in range(2):
        rows_ref[t, at.tp, rows(me), :] = send_ref[t, rows(me), :]

    def out_row(t, d):
        p = at.to(d)
        return copy_to(send_ref.at[t, rows(p)], rows_ref.at[t, at.tp, rows(me)],
                       zs.at[t, d], zr.at[t, d], {"sp": p})

    def in_row(t, d):
        p = at.source(d)
        here = rows_ref.at[t, at.tp, rows(p)]
        return copy_to(here, here, zs.at[t, d], zr.at[t, d], {"sp": p})

    def across(t, d, dy):
        here = rows_ref.at[t, at.tp, rows(at.source(d))]
        return copy_to(here, here, ys.at[t, dy, d], yr.at[t, dy, d], {"tp": at.to_chip(dy)})

    def across_in(t, d, dy):
        here = rows_ref.at[t, at.from_chip(dy), rows(at.source(d))]
        return copy_to(here, here, ys.at[t, dy, d], yr.at[t, dy, d], {"tp": at.from_chip(dy)})

    def relay(t, d, dy):
        here = rows_ref.at[t, at.from_chip(dy), rows(at.source(d))]
        return copy_to(here, here, ps.at[t, dy, d], pr.at[t, dy, d], {"tp": at.mate})

    def relay_in(t, d, dy):
        here = rows_ref.at[t, at.mate_from_chip(dy), rows(at.source(d))]
        return copy_to(here, here, ps.at[t, dy, d], pr.at[t, dy, d], {"tp": at.mate})

    def pass_on(t, d):
        @pl.when(d > 0)
        def _():
            in_row(t, d).wait_recv()
        for dy in range(1, at.chips):
            across(t, d, dy).start()
        relay(t, d, 0).start()

    def pass_mate(t, d):
        for dy in range(1, at.chips):
            across_in(t, d, dy).wait_recv()
            relay(t, d, dy).start()

    def gathered(t, d):
        for dy in range(at.chips):
            relay_in(t, d, dy).wait_recv()

    at.met()
    for t in range(2):
        loop(n - 1, lambda i, t=t: out_row(t, i + 1).start())

    for load in loads[4:10]:
        load.wait()

    pre = pre_ref[...].astype(F32)
    log_sig = jnp.minimum(pre, 0.0) - jnp.log1p(jnp.exp(-jnp.abs(pre)))
    decays = as_column(speed_ref[...]) * log_sig + extra_ref[...]
    cum_ref[...] = exact_dot(decays, triangle(tok, lambda a, b: a <= b).astype(F32))

    per_head = -(-n // heads)

    def head(h):
        keys = pl.ds(pl.multiple_of(h * KEY_DIM, KEY_DIM), KEY_DIM)
        values = pl.ds(pl.multiple_of(h * VAL_DIM, VAL_DIM), VAL_DIM)
        q = q_ref[keys, :].astype(F32) * KEY_DIM ** (-0.5)
        cum = cum_ref[keys, :]
        cum_t = cum.T
        k_t = k_ref[keys, :].astype(F32).T
        total = jnp.zeros((tok, tok), F32)
        for c in range(KEY_DIM):
            decay = jnp.exp(-jnp.abs(cum_t[:, c:c + 1] - cum[c:c + 1, :]))
            total = total + (k_t[:, c:c + 1] * q[c:c + 1, :]) * decay
        scores = total.astype(BF16)
        st_ref[pl.ds(pl.multiple_of(h * tok, tok), tok), :] = scores
        inner_ref[values, :] = dot(v_ref[values, :], scores, NN)

        def forward(i):
            @pl.when(h * per_head + i < n)
            def _():
                pass_on(0, h * per_head + i)
        loop(per_head, forward)

    loop(heads, head)

    cum = cum_ref[...]
    last = cum[:, tok - 1:tok]
    k = k_ref[...].astype(F32)
    sbuf[0] = own_heads(dot(v_ref[...], k * jnp.exp(last - cum), NT), VAL_DIM).astype(BF16)
    sbuf[1] = own_heads(dot(v_ref[...], k * jnp.exp(cum), NT), VAL_DIM).astype(BF16)
    lbuf[...] = jnp.broadcast_to(as_row(last), lbuf.shape)
    sin[me] = jnp.zeros(sin.shape[1:], BF16)
    last_ref[me] = jnp.zeros(last_ref.shape[1:], F32)

    def out_state(d):
        p = at.to(d)
        return (copy_to(sbuf.at[jnp.where(p > me, 0, 1)], sin.at[me], ss.at[0, d], sr.at[0, d],
                        {"sp": p}),
                copy_to(lbuf, last_ref.at[me], ss.at[1, d], sr.at[1, d], {"sp": p}))

    def in_state(d):
        p = at.source(d)
        return (copy_to(sbuf.at[0], sin.at[p], ss.at[0, d], sr.at[0, d], {"sp": p}),
                copy_to(lbuf, last_ref.at[p], ss.at[1, d], sr.at[1, d], {"sp": p}))

    loop(n - 1, lambda i: [copy.start() for copy in out_state(i + 1)] and None)

    half = n // 2
    loop(n, lambda d: pass_mate(0, d))
    loop(half, lambda d: pass_on(1, d))
    loop(n, lambda d: gathered(0, d))

    def columns_of(weights, t):
        total = None
        for j in range(m):
            part = dot(rows_ref[t, j], weights[j * width:(j + 1) * width, :], NN)
            total = part if total is None else total + part
        return total

    loads[10].wait()
    gp_ref[...] = columns_of(gate_v, 0)
    loop(n - half, lambda d: pass_on(1, d + half))
    loads[11].wait()
    up_ref[...] = columns_of(up_v, 0)
    loop(n, lambda d: pass_mate(1, d))

    loop(n - 1, lambda i: [copy.wait_recv() for copy in in_state(i + 1)] and None)
    before, after = carry(n, me, lambda i: sin[i].astype(F32),
                          lambda i: jnp.exp(last_ref[i, 0:1, :]))
    carried_ref[0] = before
    carried_ref[1] = after
    q = q_ref[...].astype(F32) * KEY_DIM ** (-0.5)
    mixed = inner_ref[...] + dot(spread_heads(before, heads), q * jnp.exp(cum), NN)
    mixed = mixed + dot(spread_heads(after, heads), q * jnp.exp(last - cum), NN)
    for h in range(heads):
        part = mixed[h * VAL_DIM:(h + 1) * VAL_DIM]
        inv = lax.rsqrt(jnp.mean(part * part, axis=0, keepdims=True) + 1e-06)
        normed = part * inv
        normed_ref[h * VAL_DIM:(h + 1) * VAL_DIM, :] = normed
        mix_ref[h * VAL_DIM:(h + 1) * VAL_DIM, :] = normed.astype(BF16)
        inv_ref[h * 8:(h + 1) * 8, :] = jnp.broadcast_to(inv, (8, tok))

    loop(n, lambda d: gathered(1, d))
    loads[12].wait()
    grad_hidden = None
    for j in range(m):
        part = dot(rows_ref[1, j], down_v[:, j * width:(j + 1) * width], NT)
        grad_hidden = part if grad_hidden is None else grad_hidden + part
    gate_pre, up_pre = gp_ref[...], up_ref[...]
    gate_sig = jax.nn.sigmoid(gate_pre)
    gate_act = gate_pre * gate_sig
    hidden_ref[...] = (gate_act * up_pre).astype(BF16)
    ggp_ref[...] = (grad_hidden * up_pre * gate_sig
                    * (1.0 + gate_pre * (1.0 - gate_sig))).astype(BF16)
    gup_ref[...] = (grad_hidden * gate_act).astype(BF16)

    def drain(i):
        for copy in out_state(i + 1):
            copy.wait_send()
        for t in range(2):
            out_row(t, i + 1).wait_send()
    loop(n - 1, drain)

    def drain_passed(d):
        for t in range(2):
            for dy in range(1, at.chips):
                across(t, d, dy).wait_send()
            for dy in range(at.chips):
                relay(t, d, dy).wait_send()
    loop(n, drain_passed)


def in_hbm(array):
    return pltpu.with_memory_space_constraint(array, pltpu.HBM)


def vmem_specs(count):
    return [pl.BlockSpec(memory_space=pltpu.VMEM)] * count


def dispatch(n, m, cap, q, k, v, pre, extra, speed, x, cot, picks, comb, gate, up, down):
    channels, tok = q.shape
    values = v.shape[0]
    heads = channels // KEY_DIM
    slots, width, units = n * cap, x.shape[1], gate.shape[1]
    chips = m // CORES
    dma = pltpu.SemaphoreType.DMA
    outs = [((2, m, slots, width), BF16), ((slots, units), BF16), ((slots, units), BF16),
            ((slots, units), BF16), ((slots, tok), BF16), ((heads * tok, tok), BF16),
            ((channels, tok), F32), ((values, tok), F32), ((heads * 8, tok), F32),
            ((values, tok), BF16), ((2, VAL_DIM, channels), F32), ((n, 8, channels), F32),
            (gate.shape, BF16), (up.shape, BF16)]
    outs += [(a.shape, a.dtype) for a in (q, k, v, pre, speed, cot)]
    return pl.pallas_call(
        functools.partial(dispatch_kernel, n, m, cap),
        in_specs=[pl.BlockSpec(memory_space=pltpu.HBM)] * 13,
        out_specs=vmem_specs(len(outs)),
        out_shape=[pltpu.VMEM(shape, dtype) for shape, dtype in outs],
        scratch_shapes=[
            pltpu.VMEM(extra.shape, extra.dtype), pltpu.VMEM(x.shape, x.dtype),
            pltpu.VMEM(picks.shape, picks.dtype), pltpu.VMEM(comb.shape, comb.dtype),
            pltpu.VMEM((2, slots, width), BF16), pltpu.VMEM((2, VAL_DIM, channels), BF16),
            pltpu.VMEM((n, VAL_DIM, channels), BF16), pltpu.VMEM((8, channels), F32),
            pltpu.VMEM((values, tok), F32),
            pltpu.VMEM(down.shape, BF16),
            pltpu.VMEM((slots, units), F32), pltpu.VMEM((slots, units), F32),
            dma((2, n)), dma((2, n)), dma((2, chips, n)), dma((2, chips, n)),
            dma((2, chips, n)), dma((2, chips, n)), dma((2, n)), dma((2, n)), dma((13,)),
        ],
        compiler_params=pltpu.CompilerParams(collective_id=0, has_side_effects=True,
                                             vmem_limit_bytes=VMEM_LIMIT),
        name="dispatch",
    )(*map(in_hbm, (q, k, v, pre, extra, speed, x, cot, picks, comb, gate, up, down)))


def combine_kernel(n, m, cap, rows_ref, hidden_ref, ggp_ref, gup_ref, place_ref, cot_ref, mix_ref,
                   gate_v, up_v,
                   full_ref, dgate_ref, dup_ref, ddown_ref, all_mix_ref,
                   own_ref, psend, pin, ybuf, yin, zbuf, ret_ref,
                   ps, pr, ys, yr, zs, zr, fs, fr, ms, mr):
    at = Peers(n, m)
    me = at.me
    width = cot_ref.shape[1]
    at.greet()
    def rows(p):
        return pl.ds(pl.multiple_of(p * cap, 16), cap)

    def partial(j):
        block = pl.ds(pl.multiple_of(j * width, width), width)
        return dot(ggp_ref[...], gate_v[block, :], NT) + dot(gup_ref[...], up_v[block, :], NT)

    def pair(dy):
        return copy_to(psend.at[dy], pin.at[dy], ps.at[dy], pr.at[dy], {"tp": at.mate})

    def column_of(dy, core):
        return lax.rem(at.chip + dy, at.chips) * CORES + core

    def across(d, dy):
        r = rows(at.to(d))
        return copy_to(ybuf.at[dy, r], yin.at[dy, r], ys.at[dy, d], yr.at[dy, d],
                       {"tp": at.to_chip(dy)})

    def across_in(d, dy):
        r = rows(at.to(d))
        return copy_to(yin.at[dy, r], yin.at[dy, r], ys.at[dy, d], yr.at[dy, d],
                       {"tp": at.from_chip(dy)})

    def back(d):
        return copy_to(zbuf.at[rows(at.to(d))], ret_ref.at[rows(me)], zs.at[d], zr.at[d],
                       {"sp": at.to(d)})

    def back_in(d):
        here = ret_ref.at[rows(at.source(d))]
        return copy_to(here, here, zs.at[d], zr.at[d], {"sp": at.source(d)})

    def mix_out(d):
        return copy_to(mix_ref, all_mix_ref.at[me], ms.at[d], mr.at[d], {"sp": at.to(d)})

    def mix_in(d):
        p = at.source(d)
        return copy_to(mix_ref, all_mix_ref.at[p], ms.at[d], mr.at[d], {"sp": p})

    all_mix_ref[me] = mix_ref[...]
    order = list(range(1, at.chips)) + [0]
    for i, dy in enumerate(order):
        psend[dy] = partial(column_of(dy, 1 - at.core)).astype(BF16)
        if i == 0:
            at.met()
        pair(dy).start()
        if i == 0:
            loop(n - 1, lambda i: mix_out(i + 1).start())
        own_ref[dy] = partial(column_of(dy, at.core))
        if dy > 0:
            pair(dy).wait_recv()
            ybuf[dy] = (own_ref[dy] + pin[dy].astype(F32)).astype(BF16)
            loop(n, lambda d, dy=dy: across(lax.rem(d + 1, n), dy).start())
    pair(0).wait_recv()
    own_ref[0] = own_ref[0] + pin[0].astype(F32)

    pieces = []
    for j in range(m):
        cols = slice(j * width, (j + 1) * width)

        def gate_piece(j=j, cols=cols):
            dgate_ref[cols, :] = dot(rows_ref[0, j], ggp_ref[...], TN).astype(BF16)

        def up_piece(j=j, cols=cols):
            dup_ref[cols, :] = dot(rows_ref[0, j], gup_ref[...], TN).astype(BF16)

        def down_piece(j=j, cols=cols):
            ddown_ref[:, cols] = dot(hidden_ref[...], rows_ref[1, j], TN).astype(BF16)
        pieces += [gate_piece, up_piece, down_piece]

    steps = n + 4
    done = 0
    for i in range(n):
        upto = len(pieces) * (i + 1) // steps
        for piece in pieces[done:upto]:
            piece()
        done = upto
        d = (i + 1) % n
        r = rows(at.to(d))
        total = own_ref[0, r, :]
        for dy in range(1, at.chips):
            across_in(d, dy).wait_recv()
            total = total + yin[dy, r, :].astype(F32)
        if d == 0:
            ret_ref[r, :] = total.astype(BF16)
        else:
            zbuf[r, :] = total.astype(BF16)
            back(d).start()
    upto = len(pieces) * (n + 2) // steps
    for piece in pieces[done:upto]:
        piece()
    loop(n - 1, lambda i: back_in(i + 1).wait_recv())
    picked = dot(place_ref[...], ret_ref[...], TN)
    full_ref[at.tp] = (cot_ref[...].astype(F32) + picked).astype(BF16)

    def share(dy):
        here = full_ref.at[at.tp]
        return copy_to(here, here, fs.at[0, dy], fr.at[0, dy],
                       {"tp": at.to_chip(dy)} if dy else {"tp": at.mate})

    def share_in(dy):
        here = full_ref.at[at.from_chip(dy) if dy else at.mate]
        return copy_to(here, here, fs.at[0, dy], fr.at[0, dy], {"tp": at.mate})

    def relay(dy):
        here = full_ref.at[at.from_chip(dy)]
        return copy_to(here, here, fs.at[1, dy], fr.at[1, dy], {"tp": at.mate})

    def relay_in(dy):
        here = full_ref.at[at.mate_from_chip(dy)]
        return copy_to(here, here, fs.at[1, dy], fr.at[1, dy], {"tp": at.mate})

    for dy in order:
        share(dy).start()
    for piece in pieces[upto:]:
        piece()
    for dy in range(1, at.chips):
        share_in(dy).wait_recv()
        relay(dy).start()
    share_in(0).wait_recv()
    for dy in range(1, at.chips):
        relay_in(dy).wait_recv()
    for dy in range(at.chips):
        pair(dy).wait_send()
        share(dy).wait_send()
    for dy in range(1, at.chips):
        relay(dy).wait_send()
        loop(n, lambda d, dy=dy: across(d, dy).wait_send())
    loop(n - 1, lambda i: back(i + 1).wait_send())
    loop(n - 1, lambda i: mix_out(i + 1).wait_send())
    loop(n - 1, lambda i: mix_in(i + 1).wait_recv())


def combine(n, m, cap, rows, hidden, ggp, gup, place, cot, mix, gate, up):
    slots, units = hidden.shape
    tok, width = cot.shape
    chips = m // CORES
    dma = pltpu.SemaphoreType.DMA
    outs = [((m, tok, width), BF16), (gate.shape, BF16), (up.shape, BF16),
            ((units, m * width), BF16), ((n,) + mix.shape, BF16)]
    return pl.pallas_call(
        functools.partial(combine_kernel, n, m, cap),
        in_specs=vmem_specs(9),
        out_specs=vmem_specs(len(outs)),
        out_shape=[pltpu.VMEM(shape, dtype) for shape, dtype in outs],
        scratch_shapes=[
            pltpu.VMEM((chips, slots, width), F32), pltpu.VMEM((chips, slots, width), BF16),
            pltpu.VMEM((chips, slots, width), BF16), pltpu.VMEM((chips, slots, width), BF16),
            pltpu.VMEM((chips, slots, width), BF16), pltpu.VMEM((slots, width), BF16),
            pltpu.VMEM((slots, width), BF16),
            dma((chips,)), dma((chips,)), dma((chips, n)), dma((chips, n)), dma((n,)), dma((n,)),
            dma((2, chips)), dma((2, chips)), dma((n,)), dma((n,)),
        ],
        compiler_params=pltpu.CompilerParams(collective_id=1, has_side_effects=True,
                                             vmem_limit_bytes=VMEM_LIMIT),
        name="combine",
    )(rows, hidden, ggp, gup, place, cot, mix, gate, up)


def finish_kernel(n, m, project, *refs):
    (full_ref, wo_ref, normed_ref, inv_ref, q_ref, k_ref, v_ref, pre_ref, speed_ref, cum_ref,
     st_ref, carried_ref, last_ref) = refs[:13]
    refs = refs[13:]
    if project:
        mix_ref, refs = refs[0], refs[1:]
    dq_ref, dk_ref, dv_ref, logit_ref = refs[:4]
    refs = refs[4:]
    if project:
        proj_ref, refs = refs[0], refs[1:]
    dm_ref, dc_ref, sbuf, sin, ss, sr = refs[:6]
    if project:
        psend, prow, zs, zr, fs, fr = refs[6:]
    at = Peers(n, m)
    me = at.me
    channels, tok = q_ref.shape
    values = v_ref.shape[0]
    heads = channels // KEY_DIM
    width = full_ref.shape[2]
    at.greet()

    def exchange(d):
        p = at.to(d)
        return copy_to(sbuf.at[jnp.where(p < me, 0, 1)], sin.at[me], ss.at[d], sr.at[d],
                       {"sp": p})

    def exchange_in(d):
        p = at.source(d)
        return copy_to(sbuf.at[0], sin.at[p], ss.at[d], sr.at[d], {"sp": p})

    gn = None
    for j in range(m):
        part = dot(full_ref[j], wo_ref[j * width:(j + 1) * width, :], NN)
        gn = part if gn is None else gn + part
    gn = gn.T
    for h in range(heads):
        block = slice(h * VAL_DIM, (h + 1) * VAL_DIM)
        normed, g = normed_ref[block, :], gn[block]
        dm_ref[block, :] = inv_ref[h * 8:h * 8 + 1, :] * (
            g - normed * jnp.mean(g * normed, axis=0, keepdims=True))
    cum = cum_ref[...]
    last = cum[:, tok - 1:tok]
    up, down = jnp.exp(cum), jnp.exp(last - cum)
    scale = KEY_DIM ** (-0.5)
    q = q_ref[...].astype(F32) * scale
    dm = dm_ref[...]
    sbuf[0] = own_heads(dot(dm, q * up, NT), VAL_DIM).astype(BF16)
    sbuf[1] = own_heads(dot(dm, q * down, NT), VAL_DIM).astype(BF16)
    sin[me] = jnp.zeros(sin.shape[1:], BF16)
    if project:
        block = proj_ref.shape[0]
        share = tok // m
        row = lax.broadcasted_iota(jnp.int32, (share, tok), 0) + at.tp * share
        chosen = (row == lax.broadcasted_iota(jnp.int32, (share, tok), 1)).astype(BF16)
        per = width // block
        for j in range(m):
            part = dot(chosen, full_ref[j], NN).astype(BF16)
            for i in range(per):
                psend[j * per + i] = part[:, i * block:(i + 1) * block]

        def share_of(j):
            return pl.ds(pl.multiple_of(j * share, 16), share)

        def rows_out(d):
            p = at.to(d)
            return copy_to(psend.at[p], prow.at[me, share_of(at.tp)], zs.at[d], zr.at[d],
                           {"sp": p})

        def rows_in(d):
            here = prow.at[at.source(d), share_of(at.tp)]
            return copy_to(here, here, zs.at[d], zr.at[d], {"sp": at.source(d)})

        def spread(dy):
            here = prow.at[:, share_of(at.tp)]
            return copy_to(here, here, fs.at[0, dy], fr.at[0, dy],
                           {"tp": at.to_chip(dy)} if dy else {"tp": at.mate})

        def spread_in(dy):
            here = prow.at[:, share_of(at.from_chip(dy) if dy else at.mate)]
            return copy_to(here, here, fs.at[0, dy], fr.at[0, dy], {"tp": at.mate})

        def relay(dy):
            here = prow.at[:, share_of(at.from_chip(dy))]
            return copy_to(here, here, fs.at[1, dy], fr.at[1, dy], {"tp": at.mate})

        def relay_in(dy):
            here = prow.at[:, share_of(at.mate_from_chip(dy))]
            return copy_to(here, here, fs.at[1, dy], fr.at[1, dy], {"tp": at.mate})

        prow[me, share_of(at.tp), :] = psend[me]
    at.met()
    loop(n - 1, lambda i: exchange(i + 1).start())
    if project:
        loop(n - 1, lambda i: rows_out(i + 1).start())

    row = lax.broadcasted_iota(jnp.int32, (tok, tok), 0)
    col = lax.broadcasted_iota(jnp.int32, (tok, tok), 1)
    sign = jnp.where(row > col, 1.0, jnp.where(row < col, -1.0, 0.0)).astype(F32)

    def head(h):
        keys = pl.ds(pl.multiple_of(h * KEY_DIM, KEY_DIM), KEY_DIM)
        vals = pl.ds(pl.multiple_of(h * VAL_DIM, VAL_DIM), VAL_DIM)
        dm, v, cum = dm_ref[vals, :], v_ref[vals, :], cum_ref[keys, :]
        q = q_ref[keys, :].astype(F32) * scale
        k = k_ref[keys, :].astype(F32)
        by_query = dot(dm, v, TN)
        by_key = dot(v, dm, TN)
        by_query_signed = by_query * sign
        by_key_signed = by_key * -sign
        cum_t, q_t, k_t = cum.T, q.T, k.T
        dq, dk, dq_signed, dk_signed = [], [], [], []
        for c in range(KEY_DIM):
            weight = jnp.exp(-jnp.abs(cum_t[:, c:c + 1] - cum[c:c + 1, :]))
            with_q = weight * q_t[:, c:c + 1]
            with_k = weight * k_t[:, c:c + 1]
            dk.append(jnp.sum(by_query * with_q, axis=0, keepdims=True))
            dk_signed.append(jnp.sum(by_query_signed * with_q, axis=0, keepdims=True))
            dq.append(jnp.sum(by_key * with_k, axis=0, keepdims=True))
            dq_signed.append(jnp.sum(by_key_signed * with_k, axis=0, keepdims=True))
        join = lambda parts: jnp.concatenate(parts, axis=0)
        dq_ref[keys, :] = join(dq)
        dk_ref[keys, :] = join(dk)
        dv_ref[vals, :] = dot(dm, st_ref[pl.ds(pl.multiple_of(h * tok, tok), tok), :], NT)
        dc_ref[keys, :] = q * join(dq_signed) - k * join(dk_signed)

    early = heads // 2
    loop(early, head)
    if project:
        loop(n - 1, lambda i: rows_in(i + 1).wait_recv())
        for dy in range(at.chips):
            spread(dy).start()
    loop(heads - early, lambda h: head(h + early))
    if project:
        for dy in range(1, at.chips):
            spread_in(dy).wait_recv()
            relay(dy).start()

    k = k_ref[...].astype(F32)
    in_fwd, in_bwd = carried_ref[0], carried_ref[1]
    d_up = dot(spread_heads(in_fwd, heads), dm, TN) * up
    d_down = dot(spread_heads(in_bwd, heads), dm, TN) * down
    dq_ref[...] = (dq_ref[...] + d_up + d_down) * scale
    dc = dc_ref[...] + q * (d_up - d_down)
    total = jnp.sum(q * d_down, axis=1, keepdims=True)

    loop(n - 1, lambda i: exchange_in(i + 1).wait_recv())
    grad_bwd, grad_fwd = carry(n, me, lambda i: sin[i].astype(F32),
                               lambda i: jnp.exp(last_ref[i, 0:1, :]))
    wide_fwd, wide_bwd = spread_heads(grad_fwd, heads), spread_heads(grad_bwd, heads)
    v = v_ref[...]
    d_down = dot(wide_fwd, v, TN) * down
    d_up = dot(wide_bwd, v, TN) * up
    dk_ref[...] = dk_ref[...] + d_down + d_up
    dv_ref[...] = dv_ref[...] + dot(wide_fwd, k * down, NN) + dot(wide_bwd, k * up, NN)
    factor = as_column(jnp.sum(grad_fwd * in_fwd + grad_bwd * in_bwd, axis=0, keepdims=True))
    total = total + jnp.sum(k * d_down, axis=1, keepdims=True) + factor * jnp.exp(last)
    dc = dc + k * (d_up - d_down)
    decay = exact_dot(dc, triangle(tok, lambda a, b: a >= b).astype(F32)) + total
    logit_ref[...] = decay * as_column(speed_ref[...]) * jax.nn.sigmoid(
        -pre_ref[...].astype(F32))

    if project:
        spread_in(0).wait_recv()
        for dy in range(1, at.chips):
            relay_in(dy).wait_recv()
        out = None
        for s in range(n):
            part = dot(mix_ref[s], prow[s], NN)
            out = part if out is None else out + part
        proj_ref[...] = out.T
        for dy in range(at.chips):
            spread(dy).wait_send()
        for dy in range(1, at.chips):
            relay(dy).wait_send()
        loop(n - 1, lambda i: rows_out(i + 1).wait_send())
    loop(n - 1, lambda i: exchange(i + 1).wait_send())


def finish(n, m, project, full, wo, normed, inv, q, k, v, pre, speed, cum, st, carried, lasts,
           all_mix):
    channels, tok = q.shape
    values = v.shape[0]
    block = wo.shape[0] // n
    chips = m // CORES
    dma = pltpu.SemaphoreType.DMA
    outs = [((channels, tok), F32), ((channels, tok), F32), ((values, tok), F32),
            ((channels, tok), F32)]
    scratch = [pltpu.VMEM((values, tok), F32), pltpu.VMEM((channels, tok), F32),
               pltpu.VMEM((2, VAL_DIM, channels), BF16), pltpu.VMEM((n, VAL_DIM, channels), BF16),
               dma((n,)), dma((n,))]
    args = [full, wo, normed, inv, q, k, v, pre, speed, cum, st, carried, lasts]
    if project:
        args.append(all_mix)
        outs.append(((block, values), F32))
        scratch += [pltpu.VMEM((n, tok // m, block), BF16), pltpu.VMEM((n, tok, block), BF16),
                    dma((n,)), dma((n,)), dma((2, chips)), dma((2, chips))]
    return pl.pallas_call(
        functools.partial(finish_kernel, n, m, project),
        in_specs=vmem_specs(len(args)),
        out_specs=vmem_specs(len(outs)),
        out_shape=[pltpu.VMEM(shape, dtype) for shape, dtype in outs],
        scratch_shapes=scratch,
        compiler_params=pltpu.CompilerParams(collective_id=2, has_side_effects=True,
                                             vmem_limit_bytes=VMEM_LIMIT),
        name="finish",
    )(*args)


def publish_kernel(*refs):
    count = len(refs) // 2
    sems = refs[-1]
    copies = [pltpu.make_async_copy(refs[i], refs[count + i], sems.at[i]) for i in range(count)]
    for copy in copies:
        copy.start()
    for copy in copies:
        copy.wait()


def publish(arrays):
    return pl.pallas_call(
        publish_kernel,
        in_specs=vmem_specs(len(arrays)),
        out_specs=[pl.BlockSpec(memory_space=pltpu.HBM)] * len(arrays),
        out_shape=[jax.ShapeDtypeStruct(a.shape, a.dtype) for a in arrays],
        scratch_shapes=[pltpu.SemaphoreType.DMA((len(arrays),))],
        compiler_params=pltpu.CompilerParams(vmem_limit_bytes=1 << 20),
        name="publish",
    )(*[pltpu.with_memory_space_constraint(a, pltpu.VMEM) for a in arrays])


def body(
    queries,
    input_key_matrix,
    input_value_matrix,
    decay_preactivation,
    extra_log_decay,
    channel_decay_speed,
    output_weight_matrix,
    stored_expert_rows,
    chosen_expert_index,
    expert_combine_weight,
    cotangent,
    expert_gate_weight,
    expert_up_weight,
    expert_down_weight,
):
    heads = input_value_matrix.shape[0] // VAL_DIM
    tok_rows = queries.shape[1]
    experts, m = lax.axis_size("sp"), lax.axis_size("tp")
    capacity = -(-(3 * tok_rows // experts) // 16) * 16
    slots = experts * capacity
    part_width = stored_expert_rows.shape[1]
    gate_local, up_local, down_local = expert_gate_weight[0], expert_up_weight[0], expert_down_weight[0]
    (rows, hidden, grad_gate_pre, grad_up_pre, place, scores, cum, normed, inv_rms, mix_rows,
     carried, lasts, gate_held, up_held, q, k, v, pre, speed, cot) = dispatch(
        experts, m, capacity, queries, input_key_matrix, input_value_matrix,
        decay_preactivation, extra_log_decay, channel_decay_speed[None, :], stored_expert_rows,
        cotangent, chosen_expert_index.T, expert_combine_weight.T, gate_local, up_local, down_local)
    full, grad_gate, grad_up, grad_down, all_mix = combine(
        experts, m, capacity, rows, hidden, grad_gate_pre, grad_up_pre, place, cot,
        mix_rows, gate_held, up_held)
    rows_block = output_weight_matrix.shape[0] // experts
    project = (tok_rows % (16 * m) == 0 and rows_block % 128 == 0
               and part_width % rows_block == 0)
    grads = finish(
        experts, m, project, full, output_weight_matrix, normed, inv_rms, q, k, v, pre, speed,
        cum, scores, carried, lasts, all_mix)
    held = publish([*grads, grad_gate, grad_up, grad_down])
    grad_gate, grad_up, grad_down = held[-3:]
    if project:
        grad_out_proj = held[4]
    else:
        full_rows = full.swapaxes(0, 1).reshape(tok_rows, experts, rows_block)
        all_rows = lax.all_to_all(full_rows.swapaxes(0, 1), "sp", split_axis=0, concat_axis=0,
                                  tiled=True)
        grad_out_proj = jnp.einsum("str,sct->rc", all_rows, all_mix, preferred_element_type=F32)
    return (*held[:4], grad_out_proj, grad_gate[None], grad_up[None], grad_down[None])


def solution(mesh):
    in_specs = (
        P("tp", "sp"),
        P("tp", "sp"),
        P("tp", "sp"),
        P("tp", "sp"),
        P("tp", "sp"),
        P("tp"),
        P(None, "tp"),
        P("sp", "tp"),
        P("sp", None),
        P("sp", None),
        P("sp", "tp"),
        P("sp", None, "tp"),
        P("sp", None, "tp"),
        P("sp", "tp", None),
    )
    out_specs = (
        P("tp", "sp"),
        P("tp", "sp"),
        P("tp", "sp"),
        P("tp", "sp"),
        P("sp", "tp"),
        P("sp", None, "tp"),
        P("sp", None, "tp"),
        P("sp", "tp", None),
    )
    return jax.shard_map(body, mesh=mesh, in_specs=in_specs, out_specs=out_specs, check_vma=False)
```
